128 devices in a mesh: st: 64 (over z, y, x), tp: 2 (over core).
Axes of the slice: x: 4, y: 4, z: 4, core: 2. Of those that a mesh axis runs over, the one named last changes fastest.
Arguments:
- tokens: bfloat16 [49152, 2048], P('st'), may hold values from -6 to 6, as said below
- route_ids: int32 [768, 4], P('st'), may hold values from 0 to 1535, as said below
- store: bfloat16 [1536, 128, 2048], P('st'), may hold values from -6 to 6, as said below
- token_gain: float32 [2048], replicated, may hold values from 0.1 to 1.9
- store_gain: float32 [2048], replicated, may hold values from 0.1 to 1.9
- carry_weight: bfloat16 [2048, 512], P(None, 'tp'), may hold values from -0.125 to 0.125
- spatial_weight: bfloat16 [2048, 512], P(None, 'tp'), may hold values from -0.125 to 0.125
- spatial_gain: float32 [512], P('tp'), may hold values from 0.1 to 1.9
- position_mix: bfloat16 [8, 128, 128], P('tp'), may hold values from -0.5 to 0.5
- position_bias: float32 [8, 128], P('tp'), may hold values from 0.1 to 1.9
- query_weight: bfloat16 [2048, 512], P(None, 'tp'), may hold values from -0.86178639 to 0.86178639, as said below
- key_weight: bfloat16 [2048, 512], P(None, 'tp'), may hold values from -0.86178639 to 0.86178639, as said below
- read_weight: bfloat16 [2048, 512], P(None, 'tp'), may hold values from -0.125 to 0.125
- blend_weight: bfloat16 [2048, 512], P(None, 'tp'), may hold values from -0.125 to 0.125
- output_weight: bfloat16 [512, 2048], replicated, may hold values from -0.25 to 0.25
Outputs:
- mixed: bfloat16 [49152, 2048], P(('st', 'tp'))
The draws below stay inside these ranges and needn't reach their ends.
Inputs may be any that keep to these rules, and one draw needn't show every extreme that they name: `route_ids`: each entry is a passage index; passage p is held by index p // 24 of st. All entries of the spans of one index of st (aligned blocks of 12 rows) are different; they name at most 1 passage held by any one index of st, exactly 1 held by the index before their own (cyclically), and at least one held by the index half the axis away. `tokens`: Activations; in some draws the first token of some spans equals a row of a passage that the span reads. `store`: passage rows. `query_weight`: A projection matrix. `key_weight`: A projection matrix.
All inputs are finite; a program needn't handle non-finite values.
Results may differ from the reference program's by a relative error of at most 0.012.
The reference program's roundings to bfloat16 on the way count: a program that leaves them out, or rounds other values in their place, can miss the bound.
Values may be sent and summed in bfloat16 or wider, within the bound.
A program may use at most 128 MiB of HBM per device.

```python
import jax
import jax.numpy as jnp
from jax import lax

D = 2048
HEADS = 8
HEAD_DIM = 64
WIDTH = 512
BLOCK = 128
SPAN = 64
PICKS = 4
PASS_ROWS = 128
PASS_DEV = 24
TOK_DEV = 768
TOKENS = 49152
PASSAGES = 1536
CAP = 1
N_ST = 64


def store_passage(key, passage):
    passage_key = jax.random.fold_in(jax.random.fold_in(key, 5), passage)
    sample = jax.random.normal(passage_key, (PASS_ROWS, D), jnp.float32)
    return jnp.clip(sample, -6.0, 6.0)


def draw_store(key, part):
    indices = jnp.arange(PASSAGES, dtype=jnp.int32)
    return lax.map(lambda passage: store_passage(key, passage).astype(jnp.bfloat16), indices)


def route_table(key):
    base_key = jax.random.fold_in(key, 3)
    span_dev = TOK_DEV // SPAN
    wanted = span_dev * PICKS
    pool_size = N_ST * CAP
    ranks = jax.random.permutation(jax.random.fold_in(base_key, 0), N_ST)
    heat = 1 + ranks % 4
    slots = jnp.arange(pool_size, dtype=jnp.int32)
    slot_owner = slots // CAP
    slot_copy = slots % CAP

    def reader(index):
        subkeys = jax.random.split(jax.random.fold_in(base_key, index + 1), 3)
        raw_score = jax.random.randint(subkeys[0], (pool_size,), 0, 4096, dtype=jnp.int32)
        score = raw_score * heat[slot_owner] * pool_size + slots
        before = (index + N_ST - 1) % N_ST
        across = (index + N_ST // 2) % N_ST
        forced = (slot_owner == before) | (slot_owner == across) & (slot_copy == 0)
        score = jnp.where(forced, slots - pool_size, score)
        chosen = jnp.argsort(score)[:wanted]
        owner_index = slot_owner[chosen]
        offset = jax.random.randint(subkeys[1], (N_ST,), 0, PASS_DEV, dtype=jnp.int32)
        passage = owner_index * PASS_DEV + (offset[owner_index] + slot_copy[chosen]) % PASS_DEV
        shuffle = jax.random.permutation(subkeys[2], wanted)
        return passage[shuffle].reshape(span_dev, PICKS)
    table = lax.map(reader, jnp.arange(N_ST, dtype=jnp.int32))
    return table.reshape(N_ST * span_dev, PICKS).astype(jnp.int32)


def draw_route_ids(key, part):
    return route_table(key)


def draw_tokens(key, part):
    sample = jnp.clip(jax.random.normal(jax.random.fold_in(key, 9), (TOKENS, D), jnp.float32), -6.0, 6.0)
    return sample.astype(jnp.bfloat16)


def query_key_pair(key):
    base_key = jax.random.fold_in(key, 13)
    first = jnp.clip(jax.random.normal(jax.random.fold_in(base_key, 0), (D, WIDTH), jnp.float32), -6.0, 6.0)
    second = jnp.clip(jax.random.normal(jax.random.fold_in(base_key, 1), (D, WIDTH), jnp.float32), -6.0, 6.0)
    first = first * D ** (-0.5)
    second = second * D ** (-0.5)
    return (first, second)


def draw_query_weight(key, part):
    return query_key_pair(key)[0].astype(jnp.bfloat16)


def draw_key_weight(key, part):
    return query_key_pair(key)[1].astype(jnp.bfloat16)


def level_of(rng, dims, cuts, least, high):
    factor_of, own = 1.0, jax.random.fold_in(rng, 6)
    for position, blocks in cuts:
        heights = jnp.exp(jax.random.uniform(jax.random.fold_in(own, position), (blocks,), jnp.float32, least / len(cuts), high / len(cuts)))
        factor_of = factor_of * jnp.repeat(heights, dims[position] // blocks).reshape([-1 if axis == position else 1 for axis in range(len(dims))])
    return factor_of


def noise(rng, extent, deviation, most, cuts=(), held_as=jnp.bfloat16):
    drawn = jax.random.normal(rng, extent, jnp.float32) * deviation
    if len(cuts) > 0:
        drawn = level_of(rng, extent, cuts, -0.22, 0.18) * drawn
    return jnp.clip(drawn, min=-most, max=most).astype(held_as)


def setup_inputs(seed: int = 0) -> dict:
    streams_of = jax.random.split(jax.random.key(seed), 16)
    tokens = draw_tokens(jax.random.fold_in(streams_of[15], 71), 0)
    route_ids = draw_route_ids(jax.random.fold_in(streams_of[15], 71), 0)
    store = draw_store(jax.random.fold_in(streams_of[15], 71), 0)
    token_gain = jnp.clip(1.0 + 0.18 * jax.random.normal(streams_of[3], (D,), jnp.float32), 0.1, 1.9)
    store_gain = jnp.clip(1.0 + 0.18 * jax.random.normal(streams_of[4], (D,), jnp.float32), 0.1, 1.9)
    carry_weight = noise(streams_of[5], (D, WIDTH), D ** -0.5, 0.125, ((1, 2),))
    spatial_weight = noise(streams_of[6], (D, WIDTH), D ** -0.5, 0.125, ((1, 2),))
    spatial_gain = jnp.clip(1.0 + 0.18 * jax.random.normal(streams_of[7], (WIDTH,), jnp.float32), 0.1, 1.9)
    position_mix = noise(streams_of[8], (HEADS, BLOCK, BLOCK), BLOCK ** -0.5, 0.5, ((0, 2),))
    position_bias = jnp.clip(1.0 + 0.18 * jax.random.normal(streams_of[9], (HEADS, BLOCK), jnp.float32), 0.1, 1.9)
    query_weight = draw_query_weight(jax.random.fold_in(streams_of[15], 71), 0)
    key_weight = draw_key_weight(jax.random.fold_in(streams_of[15], 71), 0)
    read_weight = noise(streams_of[12], (D, WIDTH), D ** -0.5, 0.125, ((1, 2),))
    blend_weight = noise(streams_of[13], (D, WIDTH), D ** -0.5, 0.125, ((1, 2),))
    output_weight = noise(streams_of[14], (WIDTH, D), WIDTH ** -0.5, 0.25)
    return dict(tokens=tokens, route_ids=route_ids, store=store, token_gain=token_gain, store_gain=store_gain, carry_weight=carry_weight, spatial_weight=spatial_weight, spatial_gain=spatial_gain, position_mix=position_mix, position_bias=position_bias, query_weight=query_weight, key_weight=key_weight, read_weight=read_weight, blend_weight=blend_weight, output_weight=output_weight)


norm_eps = 1e-06

def rms_scaled(matrix, gain_vector):
    values = matrix.astype(jnp.float32)
    scaled = values * lax.rsqrt(lax.optimization_barrier(jnp.mean(values * values, axis=-1, keepdims=True)) + norm_eps)
    return (scaled * gain_vector.astype(jnp.float32)).astype(jnp.bfloat16)

def passage_partial(queries, key_rows, value_rows):
    score_scale = queries.shape[-1] ** (-0.5)
    scores = jnp.einsum('bthe,bplhe->bpthl', queries.astype(jnp.float32), key_rows.astype(jnp.float32)) * score_scale
    score_peak = lax.optimization_barrier(jnp.max(scores, axis=-1, keepdims=True))
    weights = jnp.exp(scores - score_peak)
    weight_total = lax.optimization_barrier(jnp.sum(weights, axis=-1))
    rounded = lax.optimization_barrier(weights.astype(jnp.bfloat16)).astype(jnp.float32)
    summed = jnp.einsum('bpthl,bplhe->bpthe', rounded, value_rows.astype(jnp.float32))
    partial_value = (summed / weight_total[..., None]).astype(jnp.bfloat16)
    return (partial_value, score_peak[..., 0] + jnp.log(weight_total))

def merge_partials(partial_value, log_total):
    level_top = lax.optimization_barrier(jnp.max(log_total, axis=1, keepdims=True))
    weights = jnp.exp(log_total - level_top)
    weight_total = lax.optimization_barrier(jnp.sum(weights, axis=1))
    summed = lax.optimization_barrier(jnp.sum(weights[..., None] * partial_value.astype(jnp.float32), axis=1))
    return summed / weight_total[..., None]

def reference(tokens, route_ids, store, token_gain, store_gain, carry_weight, spatial_weight, spatial_gain, position_mix, position_bias, query_weight, key_weight, read_weight, blend_weight, output_weight):
    row_count = tokens.shape[0]
    normed = rms_scaled(tokens, token_gain)
    carry_branch = jnp.dot(normed, carry_weight, preferred_element_type=jnp.float32)
    spatial = jax.nn.gelu(jnp.dot(normed, spatial_weight, preferred_element_type=jnp.float32), approximate=False)
    channel_mean = lax.optimization_barrier(jnp.mean(spatial, axis=-1, keepdims=True))
    channel_spread = lax.optimization_barrier(jnp.mean(spatial * spatial, axis=-1, keepdims=True)) - channel_mean * channel_mean
    spatial_in = ((spatial - channel_mean) * lax.rsqrt(channel_spread + norm_eps) * spatial_gain.astype(jnp.float32)).astype(jnp.bfloat16)
    blocks = spatial_in.reshape(row_count // BLOCK, BLOCK, HEADS, HEAD_DIM)
    mixed_blocks = jnp.einsum('hij,njhc->nihc', position_mix.astype(jnp.float32), blocks.astype(jnp.float32))
    mixed_blocks = mixed_blocks + position_bias.astype(jnp.float32).T[None, :, :, None]
    gated_mix = jax.nn.gelu(carry_branch, approximate=False) * mixed_blocks.reshape(row_count, HEADS * HEAD_DIM)

    def project(passage):
        passage_normed = rms_scaled(passage, store_gain)
        return (jnp.dot(passage_normed, key_weight, preferred_element_type=jnp.float32).astype(jnp.bfloat16), jnp.dot(passage_normed, read_weight, preferred_element_type=jnp.float32).astype(jnp.bfloat16))
    store_keys, store_values = lax.map(project, store)
    store_keys = store_keys.reshape(store.shape[0], PASS_ROWS, HEADS, HEAD_DIM)
    store_values = store_values.reshape(store.shape[0], PASS_ROWS, HEADS, HEAD_DIM)
    queries = jnp.dot(normed, query_weight, preferred_element_type=jnp.float32).astype(jnp.bfloat16)
    queries = queries.reshape(row_count // SPAN, SPAN, HEADS, HEAD_DIM)

    def attend(item):
        span_queries, picked = item
        span_keys = store_keys[picked][None]
        span_values = store_values[picked][None]
        partial_value, log_total = passage_partial(span_queries[None], span_keys, span_values)
        return merge_partials(partial_value, log_total)[0]
    memory = lax.map(attend, (queries, route_ids)).reshape(row_count, HEADS * HEAD_DIM)
    blend_gate = jax.nn.sigmoid(jnp.dot(normed, blend_weight, preferred_element_type=jnp.float32))
    mixed_rows = (gated_mix + blend_gate * memory).astype(jnp.bfloat16)
    return jnp.dot(mixed_rows, output_weight, preferred_element_type=jnp.float32).astype(jnp.bfloat16)
```

```python
import functools

import jax
import jax.numpy as jnp
from jax import lax
from jax.experimental import pallas as pl
from jax.experimental.pallas import tpu as pltpu
from jax.sharding import PartitionSpec as P

norm_eps = 1e-06
MESH = pl.DeviceIdType.MESH
SIDE = 4
N_ST = SIDE**3
GROUP = 4


def rms_scaled(matrix, gain_vector):
    values = matrix.astype(jnp.float32)
    scaled = values * lax.rsqrt(jnp.mean(values * values, axis=-1, keepdims=True) + norm_eps)
    return (scaled * gain_vector).astype(jnp.bfloat16)


def torus_shift(index, offset, sign):
    total = 0
    for unit in (1, SIDE, SIDE * SIDE):
        mine = lax.rem(lax.div(index, unit), SIDE)
        away = lax.rem(lax.div(offset, unit), SIDE)
        total = total + lax.rem(mine + (away if sign > 0 else SIDE - away), SIDE) * unit
    return total


def step_offset(step):
    return lax.rem(step * 27, N_ST)


def exchange_kernel(
    owner_ref,
    span_ref,
    local_ref,
    head_mask_ref,
    query_ref,
    key_ref,
    value_ref,
    memory_ref,
    slots,
    asked,
    parts,
    back,
    logs,
    back_logs,
    table,
    table_smem,
    send_query,
    recv_query,
    send_table,
    recv_table,
    send_part,
    recv_part,
    send_log,
    recv_log,
    local_sem,
):
    me = lax.axis_index("st")
    core = lax.axis_index("tp")
    span_length = slots.shape[1]
    width = slots.shape[2]
    head_dim = width // head_mask_ref.shape[0]
    span_count = memory_ref.shape[0]
    pick_count = owner_ref.shape[0] // span_count
    barrier = pltpu.get_barrier_semaphore()

    def greet(step, carry):
        pl.semaphore_signal(
            barrier,
            inc=1,
            device_id=(torus_shift(me, step_offset(step), 1), core),
            device_id_type=MESH,
        )
        return carry

    lax.fori_loop(1, N_ST, greet, 0)

    def fill(slot, carry):
        slots[slot] = query_ref[span_ref[slot]]
        return carry

    lax.fori_loop(0, N_ST, fill, 0)
    table[me] = local_ref[...]
    pl.semaphore_wait(barrier, N_ST - 1)

    def table_copy(peer):
        return pltpu.make_async_remote_copy(
            src_ref=local_ref,
            dst_ref=table.at[me],
            send_sem=send_table,
            recv_sem=recv_table,
            device_id=(peer, core),
            device_id_type=MESH,
        )

    def query_copy(peer):
        return pltpu.make_async_remote_copy(
            src_ref=slots.at[peer],
            dst_ref=asked.at[me],
            send_sem=send_query,
            recv_sem=recv_query.at[me],
            device_id=(peer, core),
            device_id_type=MESH,
        )

    def send_tables(step, carry):
        table_copy(torus_shift(me, step_offset(step), 1)).start()
        return carry

    lax.fori_loop(1, N_ST, send_tables, 0)

    def send_queries(step, carry):
        query_copy(torus_shift(me, step_offset(step), 1)).start()
        return carry

    lax.fori_loop(1, N_ST, send_queries, 0)
    asked[me] = slots[me]
    rest = pl.ds(0, N_ST - 1)
    pltpu.make_async_copy(table.at[rest], table.at[rest], recv_table).wait()
    copy = pltpu.make_async_copy(table, table_smem, local_sem)
    copy.start()
    copy.wait()

    def attend(source):
        index = table_smem[source, 0, me]
        keys = key_ref[index]
        values_t = value_ref[index]
        query = asked[source]
        spread = jnp.concatenate(
            [query * head_mask_ref[h] for h in range(head_mask_ref.shape[0])], axis=0
        )
        scores = lax.dot_general(
            keys, spread, (((1,), (1,)), ((), ())), preferred_element_type=jnp.float32
        ) * (head_dim**-0.5)
        peak = jnp.max(scores, axis=0, keepdims=True)
        weights = jnp.exp(scores - peak)
        total = jnp.sum(weights, axis=0, keepdims=True)
        summed = jnp.dot(values_t, weights.astype(jnp.bfloat16), preferred_element_type=jnp.float32)
        lane_head = lax.broadcasted_iota(jnp.int32, (head_dim, width), 1) // head_dim
        mine = summed[:head_dim]
        for h in range(1, head_mask_ref.shape[0]):
            mine = jnp.where(lane_head == h, summed[h * head_dim : (h + 1) * head_dim], mine)
        return (mine / total).astype(jnp.bfloat16), peak + jnp.log(total)

    def part_copy(source):
        return pltpu.make_async_remote_copy(
            src_ref=parts.at[source],
            dst_ref=back.at[me],
            send_sem=send_part,
            recv_sem=recv_part,
            device_id=(source, core),
            device_id_type=MESH,
        )

    def log_copy(source):
        return pltpu.make_async_remote_copy(
            src_ref=logs.at[source],
            dst_ref=back_logs.at[me],
            send_sem=send_log,
            recv_sem=recv_log,
            device_id=(source, core),
            device_id_type=MESH,
        )

    def send_back(step):
        source = torus_shift(me, step_offset(step), -1)
        part_copy(source).start()
        log_copy(source).start()

    def serve(group, carry):
        for j in range(GROUP):
            step = group * GROUP + j
            source = torus_shift(me, step_offset(step), -1)

            @pl.when(step > 0)
            def _():
                pltpu.make_async_copy(asked.at[source], asked.at[source], recv_query.at[source]).wait()

        for j in range(GROUP):
            step = group * GROUP + j
            source = torus_shift(me, step_offset(step), -1)
            part, log_total = attend(source)
            parts[source] = part
            logs[source] = log_total

        for j in range(GROUP):
            step = (group - 1) * GROUP + j

            @pl.when(step > 0)
            def _():
                send_back(step)

        return carry

    lax.fori_loop(0, N_ST // GROUP, serve, 0)
    for j in range(GROUP):
        send_back(N_ST - GROUP + j)
    back[me] = parts[me]
    back_logs[me] = logs[me]
    pltpu.make_async_copy(back.at[rest], back.at[rest], recv_part).wait()
    pltpu.make_async_copy(back_logs.at[rest], back_logs.at[rest], recv_log).wait()

    def merge(span, carry):
        owners = [owner_ref[span * pick_count + k] for k in range(pick_count)]
        levels = [back_logs[o] for o in owners]
        top = functools.reduce(jnp.maximum, levels)
        scales = [jnp.exp(level - top) for level in levels]
        total = functools.reduce(jnp.add, scales)
        summed = functools.reduce(
            jnp.add, [s * back[o].astype(jnp.float32) for s, o in zip(scales, owners)]
        )
        turned = (summed / total).T
        memory_ref[span] = jnp.concatenate(
            [turned[h * span_length : (h + 1) * span_length] for h in range(head_mask_ref.shape[0])],
            axis=1,
        )
        return carry

    lax.fori_loop(0, span_count, merge, 0)
    pltpu.make_async_copy(slots.at[rest], slots.at[rest], send_query).wait()
    pltpu.make_async_copy(table.at[rest], table.at[rest], send_table).wait()
    pltpu.make_async_copy(parts.at[rest], parts.at[rest], send_part).wait()
    pltpu.make_async_copy(logs.at[rest], logs.at[rest], send_log).wait()


def exchange(owner, slot_span, slot_local, queries, keys, values_t):
    span_count, span_length, width = queries.shape
    head_dim = values_t.shape[1] // 4
    heads = width // head_dim
    lanes = jnp.arange(width, dtype=jnp.int32) // head_dim
    head_mask = (lanes[None, None, :] == jnp.arange(heads, dtype=jnp.int32)[:, None, None]).astype(
        jnp.bfloat16
    )
    head_mask = jnp.broadcast_to(head_mask, (heads, span_length, width))
    block = pltpu.VMEM((N_ST, span_length, width), jnp.bfloat16)
    smem = pl.BlockSpec(memory_space=pltpu.SMEM)
    vmem = pl.BlockSpec(memory_space=pltpu.VMEM)
    return pl.pallas_call(
        exchange_kernel,
        out_shape=jax.ShapeDtypeStruct((span_count, span_length, width), jnp.float32),
        in_specs=[smem, smem] + [vmem] * 5,
        out_specs=vmem,
        scratch_shapes=[block] * 4
        + [pltpu.VMEM((N_ST, 1, width), jnp.float32)] * 2
        + [
            pltpu.VMEM((N_ST, 1, 128), jnp.int32),
            pltpu.SMEM((N_ST, 1, 128), jnp.int32),
            pltpu.SemaphoreType.DMA,
            pltpu.SemaphoreType.DMA((N_ST,)),
        ]
        + [pltpu.SemaphoreType.DMA] * 7,
        compiler_params=pltpu.CompilerParams(
            collective_id=0, has_side_effects=True, vmem_limit_bytes=40 << 20
        ),
    )(owner, slot_span, slot_local, head_mask, queries, keys, values_t)


def per_device(
    tokens,
    route_ids,
    store,
    token_gain,
    store_gain,
    carry_weight,
    spatial_weight,
    spatial_gain,
    position_mix,
    position_bias,
    query_weight,
    key_weight,
    read_weight,
    blend_weight,
    output_weight,
):
    row_count = tokens.shape[0]
    local_heads = position_mix.shape[0]
    block_length = position_mix.shape[1]
    local_width = carry_weight.shape[1]
    head_dim = local_width // local_heads
    span_count, pick_count = route_ids.shape
    span_length = row_count // span_count
    store_count, passage_length = (store.shape[0], store.shape[1])
    flat_ids = route_ids.reshape(-1)
    owner = flat_ids // store_count
    hit = owner[:, None] == jnp.arange(128, dtype=jnp.int32)[None, :]
    span_of = jnp.arange(span_count * pick_count, dtype=jnp.int32)[:, None] // pick_count
    slot_span = jnp.sum(jnp.where(hit, span_of, 0), axis=0)
    slot_local = jnp.sum(jnp.where(hit, (flat_ids % store_count)[:, None], 0), axis=0)
    store_rows = rms_scaled(store.reshape(store_count * passage_length, store.shape[2]), store_gain)
    keys = jnp.dot(store_rows, key_weight, preferred_element_type=jnp.float32).astype(jnp.bfloat16)
    keys = keys.reshape(store_count, passage_length, local_width)
    values = jnp.dot(store_rows, read_weight, preferred_element_type=jnp.float32).astype(jnp.bfloat16)
    values_t = values.reshape(store_count, passage_length, local_width).transpose(0, 2, 1)
    normed = rms_scaled(tokens, token_gain)
    queries = jnp.dot(normed, query_weight, preferred_element_type=jnp.float32).astype(jnp.bfloat16)
    queries = queries.reshape(span_count, span_length, local_width)
    memory = exchange(owner, slot_span, slot_local.reshape(1, 128), queries, keys, values_t)
    memory = memory.reshape(row_count, local_width)
    carry_branch = jnp.dot(normed, carry_weight, preferred_element_type=jnp.float32)
    spatial = jax.nn.gelu(
        jnp.dot(normed, spatial_weight, preferred_element_type=jnp.float32), approximate=False
    )
    total_width = local_width * lax.axis_size("tp")
    moment_one, moment_two = lax.psum(
        (jnp.sum(spatial, axis=1), jnp.sum(spatial * spatial, axis=1)), "tp"
    )
    channel_mean = (moment_one / total_width)[:, None]
    channel_spread = (moment_two / total_width)[:, None] - channel_mean * channel_mean
    spatial_in = (
        (spatial - channel_mean) * lax.rsqrt(channel_spread + norm_eps) * spatial_gain
    ).astype(jnp.bfloat16)
    blocks = spatial_in.reshape(row_count // block_length, block_length, local_heads, head_dim)
    mixed_blocks = jnp.einsum(
        "hij,njhc->nihc", position_mix, blocks, preferred_element_type=jnp.float32
    )
    mixed_blocks = mixed_blocks + position_bias.T[None, :, :, None]
    gated_mix = jax.nn.gelu(carry_branch, approximate=False) * mixed_blocks.reshape(
        row_count, local_width
    )
    blend_gate = jax.nn.sigmoid(jnp.dot(normed, blend_weight, preferred_element_type=jnp.float32))
    mixed_rows = (gated_mix + blend_gate * memory).astype(jnp.bfloat16)
    by_rows = lax.all_to_all(mixed_rows, "tp", split_axis=0, concat_axis=1, tiled=True)
    return jnp.dot(by_rows, output_weight, preferred_element_type=jnp.float32).astype(jnp.bfloat16)


def solution(mesh):
    in_specs = (
        P("st", None),
        P("st", None),
        P("st", None, None),
        P(),
        P(),
        P(None, "tp"),
        P(None, "tp"),
        P("tp"),
        P("tp", None, None),
        P("tp", None),
        P(None, "tp"),
        P(None, "tp"),
        P(None, "tp"),
        P(None, "tp"),
        P(),
    )
    out_specs = P(("st", "tp"), None)
    return jax.shard_map(
        per_device, mesh=mesh, in_specs=in_specs, out_specs=out_specs, check_vma=False
    )
```

```python
import functools

import jax
import jax.numpy as jnp
from jax import lax
from jax.experimental import pallas as pl
from jax.experimental.pallas import tpu as pltpu
from jax.sharding import PartitionSpec as P

norm_eps = 1e-06
MESH = pl.DeviceIdType.MESH
SIDE = 4
N_ST = SIDE**3
GROUP = 4
CHUNK = 16
TILE = 256


def torus_shift(index, offset, sign):
    total = 0
    for unit in (1, SIDE, SIDE * SIDE):
        mine = lax.rem(lax.div(index, unit), SIDE)
        away = lax.rem(lax.div(offset, unit), SIDE)
        total = total + lax.rem(mine + (away if sign > 0 else SIDE - away), SIDE) * unit
    return total


def step_offset(step):
    return lax.rem(step * 27, N_ST)


def gelu(x):
    return 0.5 * x * (1.0 + lax.erf(x * 0.5**0.5))


def norm_rows(source, target, gain_ref, count, source_base, target_base):
    features = source.shape[1]
    gain = gain_ref[...]

    def some(i, carry):
        rows = pl.ds(pl.multiple_of(source_base + i * CHUNK, CHUNK), CHUNK)
        values = source[rows, :].astype(jnp.float32)
        mean = jnp.sum(values * values, axis=1, keepdims=True) * (1.0 / features)
        scaled = values * lax.rsqrt(mean + norm_eps) * gain
        rows = pl.ds(pl.multiple_of(target_base + i * CHUNK, CHUNK), CHUNK)
        target[rows, :] = scaled.astype(jnp.bfloat16)
        return carry

    lax.fori_loop(0, count // CHUNK, some, 0, unroll=4)


def layer_kernel(
    ids_smem,
    ids_ref,
    tokens_hbm,
    store_hbm,
    token_gain_hbm,
    store_gain_hbm,
    carry_weight_hbm,
    spatial_weight_hbm,
    spatial_gain_hbm,
    position_mix_hbm,
    position_bias_hbm,
    query_weight_hbm,
    key_weight_hbm,
    read_weight_hbm,
    blend_weight_hbm,
    out_ref,
    tokens,
    store,
    token_gain,
    store_gain,
    carry_weight,
    spatial_weight,
    spatial_gain,
    position_mix,
    position_bias,
    query_weight,
    key_weight,
    read_weight,
    blend_weight,
    rows_normed,
    head_mask,
    queries,
    keys,
    values_t,
    slots,
    asked,
    parts,
    back,
    logs,
    back_logs,
    span_row,
    span_smem,
    local_row,
    table,
    table_smem,
    gated,
    spatial,
    blend,
    moments,
    other_moments,
    mixed,
    other_mixed,
    load_tokens,
    load_store,
    load_small,
    send_query,
    recv_query,
    send_table,
    recv_table,
    send_part,
    recv_part,
    send_log,
    recv_log,
    send_moments,
    recv_moments,
    send_mixed,
    recv_mixed,
    span_sem,
    table_sem,
):
    me = lax.axis_index("st")
    core = lax.axis_index("tp")
    span_count, pick_count = ids_ref.shape
    span_length, width = slots.shape[1:]
    passage_count, passage_length = keys.shape[:2]
    heads, block_length = position_bias.shape
    head_dim = width // heads
    row_count = tokens.shape[0]
    half = row_count // 2
    barrier = pltpu.get_barrier_semaphore()

    def greet(step, carry):
        pl.semaphore_signal(
            barrier,
            inc=1,
            device_id=(torus_shift(me, step_offset(step), 1), core),
            device_id_type=MESH,
        )
        return carry

    lax.fori_loop(1, N_ST, greet, 0)
    pl.semaphore_signal(barrier, inc=1, device_id=(me, 1 - core), device_id_type=MESH)

    def tile_rows(i, size):
        return pl.ds(pl.multiple_of(i * size, size), size)

    def token_load(i):
        rows = tile_rows(i, TILE)
        return pltpu.make_async_copy(tokens_hbm.at[rows], tokens.at[rows], load_tokens.at[i])

    def store_load(i):
        rows = tile_rows(i, TILE)
        return pltpu.make_async_copy(store_hbm.at[rows], store.at[rows], load_store.at[i])

    small = {}
    for n, (name, source, target) in enumerate(
        (
            ("token_gain", token_gain_hbm, token_gain),
            ("query_weight", query_weight_hbm, query_weight),
            ("store_gain", store_gain_hbm, store_gain),
            ("key_weight", key_weight_hbm, key_weight),
            ("read_weight", read_weight_hbm, read_weight),
            ("spatial_weight", spatial_weight_hbm, spatial_weight),
            ("spatial_gain", spatial_gain_hbm, spatial_gain),
            ("carry_weight", carry_weight_hbm, carry_weight),
            ("blend_weight", blend_weight_hbm, blend_weight),
            ("position_mix", position_mix_hbm, position_mix),
            ("position_bias", position_bias_hbm, position_bias),
        )
    ):
        small[name] = pltpu.make_async_copy(source, target, load_small.at[n])
    small["token_gain"].start()
    token_tiles = row_count // TILE
    store_tiles = store.shape[0] // TILE
    for i in range(token_tiles):
        token_load(i).start()
    small["query_weight"].start()
    small["store_gain"].start()
    small["key_weight"].start()
    small["read_weight"].start()
    for i in range(store_tiles):
        store_load(i).start()
    for name in (
        "spatial_weight",
        "spatial_gain",
        "carry_weight",
        "blend_weight",
        "position_mix",
        "position_bias",
    ):
        small[name].start()

    ids = ids_ref[...]
    lane = lax.broadcasted_iota(jnp.int32, (span_count, 128), 1) * passage_count
    span_index = lax.broadcasted_iota(jnp.int32, (span_count, 128), 0)
    slot_span = jnp.zeros((span_count, 128), jnp.int32)
    slot_local = jnp.zeros((span_count, 128), jnp.int32)
    for k in range(pick_count):
        local = ids[:, k : k + 1] - lane
        hit = (local >= 0) & (local < passage_count)
        slot_span = slot_span + jnp.where(hit, span_index, 0)
        slot_local = slot_local + jnp.where(hit, local, 0)
    slot_span = jnp.sum(slot_span, axis=0, keepdims=True)
    slot_local = jnp.sum(slot_local, axis=0, keepdims=True)
    span_row[...] = jnp.minimum(slot_span, span_count - 1)
    local_row[...] = jnp.minimum(slot_local, passage_count - 1)
    table[me] = local_row[...]
    mask_lane = lax.broadcasted_iota(jnp.int32, (span_length, width), 1) // head_dim
    for h in range(heads):
        head_mask[h] = jnp.where(mask_lane == h, 1.0, 0.0).astype(jnp.bfloat16)
    span_copy = pltpu.make_async_copy(span_row, span_smem, span_sem)
    span_copy.start()

    small["token_gain"].wait()

    def token_norm(i, carry):
        token_load(i).wait()
        norm_rows(tokens, tokens, token_gain, TILE, i * TILE, i * TILE)
        return carry

    lax.fori_loop(0, token_tiles, token_norm, 0)
    small["query_weight"].wait()

    def token_query(i, carry):
        found = jnp.dot(
            tokens[tile_rows(i, TILE), :], query_weight[...], preferred_element_type=jnp.float32
        ).astype(jnp.bfloat16)
        spans = TILE // span_length
        for s in range(spans):
            queries[i * spans + s] = found[s * span_length : (s + 1) * span_length]
        return carry

    lax.fori_loop(0, token_tiles, token_query, 0)
    span_copy.wait()

    def fill(slot, carry):
        slots[slot] = queries[span_smem[0, slot]]
        return carry

    lax.fori_loop(0, N_ST, fill, 0, unroll=4)
    pl.semaphore_wait(barrier, N_ST)

    def table_copy(peer):
        return pltpu.make_async_remote_copy(
            src_ref=local_row,
            dst_ref=table.at[me],
            send_sem=send_table,
            recv_sem=recv_table,
            device_id=(peer, core),
            device_id_type=MESH,
        )

    def query_copy(peer):
        return pltpu.make_async_remote_copy(
            src_ref=slots.at[peer],
            dst_ref=asked.at[me],
            send_sem=send_query,
            recv_sem=recv_query.at[me],
            device_id=(peer, core),
            device_id_type=MESH,
        )

    def send_tables(step, carry):
        table_copy(torus_shift(me, step_offset(step), 1)).start()
        return carry

    lax.fori_loop(1, N_ST, send_tables, 0)

    def send_queries(step, carry):
        query_copy(torus_shift(me, step_offset(step), 1)).start()
        return carry

    lax.fori_loop(1, N_ST, send_queries, 0)
    asked[me] = slots[me]

    small["store_gain"].wait()
    small["key_weight"].wait()
    small["read_weight"].wait()

    def project(i, carry):
        store_load(i).wait()
        norm_rows(store, rows_normed, store_gain, TILE, i * TILE, 0)
        rows = rows_normed[...]
        key_rows = jnp.dot(rows, key_weight[...], preferred_element_type=jnp.float32)
        value_rows = jnp.dot(rows, read_weight[...], preferred_element_type=jnp.float32)
        several = TILE // passage_length
        for p in range(several):
            part = slice(p * passage_length, (p + 1) * passage_length)
            keys[i * several + p] = key_rows[part].astype(jnp.bfloat16)
            values_t[i * several + p] = value_rows[part].T.astype(jnp.bfloat16)
        return carry

    lax.fori_loop(0, store_tiles, project, 0)

    rest = pl.ds(0, N_ST - 1)
    pltpu.make_async_copy(table.at[rest], table.at[rest], recv_table).wait()
    table_read = pltpu.make_async_copy(table, table_smem, table_sem)
    table_read.start()
    table_read.wait()

    def attend(source):
        index = table_smem[source, 0, me]
        query = asked[source]
        spread = jnp.concatenate([query * head_mask[h] for h in range(heads)], axis=0)
        scores = lax.dot_general(
            keys[index], spread, (((1,), (1,)), ((), ())), preferred_element_type=jnp.float32
        ) * (head_dim**-0.5)
        peak = jnp.max(scores, axis=0, keepdims=True)
        weights = jnp.exp(scores - peak)
        total = jnp.sum(weights, axis=0, keepdims=True)
        summed = jnp.dot(
            values_t[index], weights.astype(jnp.bfloat16), preferred_element_type=jnp.float32
        )
        mine = summed[:head_dim]
        for h in range(1, heads):
            mine = jnp.where(mask_lane == h, summed[h * head_dim : (h + 1) * head_dim], mine)
        return (mine / total).astype(jnp.bfloat16), peak + jnp.log(total)

    def part_copy(source):
        return pltpu.make_async_remote_copy(
            src_ref=parts.at[source],
            dst_ref=back.at[me],
            send_sem=send_part,
            recv_sem=recv_part,
            device_id=(source, core),
            device_id_type=MESH,
        )

    def log_copy(source):
        return pltpu.make_async_remote_copy(
            src_ref=logs.at[source],
            dst_ref=back_logs.at[me],
            send_sem=send_log,
            recv_sem=recv_log,
            device_id=(source, core),
            device_id_type=MESH,
        )

    def send_back(step):
        source = torus_shift(me, step_offset(step), -1)
        part_copy(source).start()
        log_copy(source).start()

    def serve(group, carry):
        for j in range(GROUP):
            step = group * GROUP + j
            source = torus_shift(me, step_offset(step), -1)

            @pl.when(step > 0)
            def _():
                pltpu.make_async_copy(asked.at[source], asked.at[source], recv_query.at[source]).wait()

        for j in range(GROUP):
            source = torus_shift(me, step_offset(group * GROUP + j), -1)
            part, log_total = attend(source)
            parts[source] = part
            logs[source] = log_total

        for j in range(GROUP):
            step = (group - 1) * GROUP + j

            @pl.when(step > 0)
            def _():
                send_back(step)

        return carry

    lax.fori_loop(0, N_ST // GROUP, serve, 0)
    for j in range(GROUP):
        send_back(N_ST - GROUP + j)
    back[me] = parts[me]
    back_logs[me] = logs[me]

    small["spatial_weight"].wait()
    moment_lane = lax.broadcasted_iota(jnp.int32, (TILE, 128), 1)

    def spatial_tile(i, carry):
        rows = tile_rows(i, TILE)
        found = gelu(
            jnp.dot(tokens[rows, :], spatial_weight[...], preferred_element_type=jnp.float32)
        )
        spatial[rows, :] = found
        one = jnp.sum(found, axis=1, keepdims=True)
        two = jnp.sum(found * found, axis=1, keepdims=True)
        moments[rows, :] = jnp.where(moment_lane < 64, one, two)
        return carry

    lax.fori_loop(0, token_tiles, spatial_tile, 0)
    small["carry_weight"].wait()
    small["blend_weight"].wait()

    def carry_tile(i, carry):
        rows = tile_rows(i, TILE)
        gated[rows, :] = gelu(
            jnp.dot(tokens[rows, :], carry_weight[...], preferred_element_type=jnp.float32)
        )
        blend[rows, :] = jax.nn.sigmoid(
            jnp.dot(tokens[rows, :], blend_weight[...], preferred_element_type=jnp.float32)
        )
        return carry

    moment_copy = pltpu.make_async_remote_copy(
        src_ref=moments,
        dst_ref=other_moments,
        send_sem=send_moments,
        recv_sem=recv_moments,
        device_id=(me, 1 - core),
        device_id_type=MESH,
    )
    moment_copy.start()
    lax.fori_loop(0, token_tiles, carry_tile, 0)
    small["spatial_gain"].wait()
    small["position_mix"].wait()
    small["position_bias"].wait()
    moment_copy.wait()
    block_head = lax.broadcasted_iota(jnp.int32, (block_length, width), 1) // head_dim
    bias_columns = jnp.concatenate([position_bias[...]] * (8 // heads), axis=0).T
    bias = jnp.zeros((block_length, width), jnp.float32)
    for h in range(heads):
        bias = jnp.where(block_head == h, bias_columns[:, h : h + 1], bias)

    def mix_block(i, carry):
        rows = tile_rows(i, block_length)
        both = (moments[rows, :] + other_moments[rows, :]) * (0.5 / width)
        mean = both[:, :1]
        spread = both[:, 64:65] - mean * mean
        fed = (
            (spatial[rows, :] - mean) * lax.rsqrt(spread + norm_eps) * spatial_gain[...]
        ).astype(jnp.bfloat16)
        every = jnp.dot(position_mix[...], fed, preferred_element_type=jnp.float32)
        found = every[:block_length]
        for h in range(1, heads):
            found = jnp.where(
                block_head == h, every[h * block_length : (h + 1) * block_length], found
            )
        gated[rows, :] = gated[rows, :] * (found + bias)
        return carry

    lax.fori_loop(0, row_count // block_length, mix_block, 0)

    pltpu.make_async_copy(back.at[rest], back.at[rest], recv_part).wait()
    pltpu.make_async_copy(back_logs.at[rest], back_logs.at[rest], recv_log).wait()

    def merge(span):
        owners = [lax.div(ids_smem[span, k], passage_count) for k in range(pick_count)]
        levels = [back_logs[o] for o in owners]
        top = functools.reduce(jnp.maximum, levels)
        scales = [jnp.exp(level - top) for level in levels]
        total = functools.reduce(jnp.add, scales)
        summed = functools.reduce(
            jnp.add, [s * back[o].astype(jnp.float32) for s, o in zip(scales, owners)]
        )
        turned = (summed / total).T
        memory = jnp.concatenate(
            [turned[h * span_length : (h + 1) * span_length] for h in range(heads)], axis=1
        )
        rows = tile_rows(span, span_length)
        mixed[rows, :] = (gated[rows, :] + blend[rows, :] * memory).astype(jnp.bfloat16)

    def merge_half(first):
        def some(i, carry):
            merge(first + 2 * i)
            merge(first + 2 * i + 1)
            return carry

        lax.fori_loop(0, span_count // 4, some, 0)

    merge_half((1 - core) * (span_count // 2))
    mixed_copy = pltpu.make_async_remote_copy(
        src_ref=mixed.at[tile_rows(1 - core, half)],
        dst_ref=other_mixed,
        send_sem=send_mixed,
        recv_sem=recv_mixed,
        device_id=(me, 1 - core),
        device_id_type=MESH,
    )
    mixed_copy.start()
    merge_half(core * (span_count // 2))
    mine = tile_rows(core, half)

    @pl.when(core == 0)
    def _():
        out_ref[:, :width] = mixed[mine, :]

    @pl.when(core == 1)
    def _():
        out_ref[:, width:] = mixed[mine, :]

    mixed_copy.wait()

    @pl.when(core == 0)
    def _():
        out_ref[:, width:] = other_mixed[...]

    @pl.when(core == 1)
    def _():
        out_ref[:, :width] = other_mixed[...]

    pltpu.make_async_copy(slots.at[rest], slots.at[rest], send_query).wait()
    pltpu.make_async_copy(table.at[rest], table.at[rest], send_table).wait()
    pltpu.make_async_copy(parts.at[rest], parts.at[rest], send_part).wait()
    pltpu.make_async_copy(logs.at[rest], logs.at[rest], send_log).wait()


def per_device(
    tokens,
    route_ids,
    store,
    token_gain,
    store_gain,
    carry_weight,
    spatial_weight,
    spatial_gain,
    position_mix,
    position_bias,
    query_weight,
    key_weight,
    read_weight,
    blend_weight,
    output_weight,
):
    row_count, features = tokens.shape
    heads, block_length = position_mix.shape[:2]
    width = carry_weight.shape[1]
    span_count = route_ids.shape[0]
    span_length = row_count // span_count
    passage_count, passage_length = store.shape[:2]
    store = store.reshape(passage_count * passage_length, features)
    token_gain = token_gain.reshape(1, features)
    store_gain = store_gain.reshape(1, features)
    spatial_gain = spatial_gain.reshape(1, width)
    position_mix = position_mix.reshape(heads * block_length, block_length)
    bf16, f32 = jnp.bfloat16, jnp.float32
    block = pltpu.VMEM((N_ST, span_length, width), bf16)
    weight = pltpu.VMEM((features, width), bf16)
    by_row = pltpu.VMEM((row_count, width), f32)
    dma = pltpu.SemaphoreType.DMA
    anywhere = pl.BlockSpec(memory_space=pl.ANY)
    by_rows = pl.pallas_call(
        layer_kernel,
        out_shape=jax.ShapeDtypeStruct((row_count // 2, 2 * width), bf16),
        in_specs=[
            pl.BlockSpec(memory_space=pltpu.SMEM),
            pl.BlockSpec(memory_space=pltpu.VMEM),
        ]
        + [anywhere] * 13,
        out_specs=pl.BlockSpec(memory_space=pltpu.VMEM),
        scratch_shapes=[
            pltpu.VMEM(tokens.shape, bf16),
            pltpu.VMEM(store.shape, bf16),
            pltpu.VMEM((1, features), f32),
            pltpu.VMEM((1, features), f32),
            weight,
            weight,
            pltpu.VMEM((1, width), f32),
            pltpu.VMEM(position_mix.shape, bf16),
            pltpu.VMEM(position_bias.shape, f32),
            weight,
            weight,
            weight,
            weight,
            pltpu.VMEM((TILE, features), bf16),
            pltpu.VMEM((heads, span_length, width), bf16),
            pltpu.VMEM((span_count, span_length, width), bf16),
            pltpu.VMEM((passage_count, passage_length, width), bf16),
            pltpu.VMEM((passage_count, width, passage_length), bf16),
            block,
            block,
            block,
            block,
            pltpu.VMEM((N_ST, 1, width), f32),
            pltpu.VMEM((N_ST, 1, width), f32),
            pltpu.VMEM((1, 128), jnp.int32),
            pltpu.SMEM((1, 128), jnp.int32),
            pltpu.VMEM((1, 128), jnp.int32),
            pltpu.VMEM((N_ST, 1, 128), jnp.int32),
            pltpu.SMEM((N_ST, 1, 128), jnp.int32),
            by_row,
            by_row,
            by_row,
            pltpu.VMEM((row_count, 128), f32),
            pltpu.VMEM((row_count, 128), f32),
            pltpu.VMEM((row_count, width), bf16),
            pltpu.VMEM((row_count // 2, width), bf16),
            dma((row_count // TILE,)),
            dma((store.shape[0] // TILE,)),
            dma((11,)),
            dma,
            dma((N_ST,)),
        ]
        + [dma] * 12,
        compiler_params=pltpu.CompilerParams(
            collective_id=0, has_side_effects=True, vmem_limit_bytes=60 << 20
        ),
    )(
        route_ids,
        route_ids,
        tokens,
        store,
        token_gain,
        store_gain,
        carry_weight,
        spatial_weight,
        spatial_gain,
        position_mix,
        position_bias,
        query_weight,
        key_weight,
        read_weight,
        blend_weight,
    )
    return jnp.dot(by_rows, output_weight, preferred_element_type=f32).astype(bf16)


def solution(mesh):
    in_specs = (
        P("st", None),
        P("st", None),
        P("st", None, None),
        P(),
        P(),
        P(None, "tp"),
        P(None, "tp"),
        P("tp"),
        P("tp", None, None),
        P("tp", None),
        P(None, "tp"),
        P(None, "tp"),
        P(None, "tp"),
        P(None, "tp"),
        P(),
    )
    out_specs = P(("st", "tp"), None)
    return jax.shard_map(
        per_device, mesh=mesh, in_specs=in_specs, out_specs=out_specs, check_vma=False
    )
```

```python
import functools

import jax
import jax.numpy as jnp
from jax import lax
from jax.experimental import pallas as pl
from jax.experimental.pallas import tpu as pltpu
from jax.sharding import PartitionSpec as P

norm_eps = 1e-06
MESH = pl.DeviceIdType.MESH
SIDE = 4
N_ST = SIDE**3
GROUP = 4
CHUNK = 16
TILE = 256


OFFSETS = [
    ((b + j) % SIDE, (a + j) % SIDE, j)
    for a in range(SIDE)
    for b in range(SIDE)
    for j in range(SIDE)
]


def gelu(x):
    return 0.5 * x * (1.0 + lax.erf(x * 0.5**0.5))


def norm_rows(source, target, gain_ref, count, source_base, target_base, unroll=4):
    features = source.shape[1]
    gain = gain_ref[...]

    def some(i, carry):
        rows = pl.ds(pl.multiple_of(source_base + i * CHUNK, CHUNK), CHUNK)
        values = source[rows, :].astype(jnp.float32)
        mean = jnp.sum(values * values, axis=1, keepdims=True) * (1.0 / features)
        scaled = values * lax.rsqrt(mean + norm_eps) * gain
        rows = pl.ds(pl.multiple_of(target_base + i * CHUNK, CHUNK), CHUNK)
        target[rows, :] = scaled.astype(jnp.bfloat16)
        return carry

    lax.fori_loop(0, count // CHUNK, some, 0, unroll=unroll)


def layer_kernel(
    ids_smem,
    ids_ref,
    tokens_hbm,
    store_hbm,
    token_gain_hbm,
    store_gain_hbm,
    carry_weight_hbm,
    spatial_weight_hbm,
    spatial_gain_hbm,
    position_mix_hbm,
    position_bias_hbm,
    query_weight_hbm,
    key_weight_hbm,
    read_weight_hbm,
    blend_weight_hbm,
    out_ref,
    tokens,
    store,
    token_gain,
    store_gain,
    carry_weight,
    spatial_weight,
    spatial_gain,
    position_mix,
    position_bias,
    query_weight,
    key_weight,
    read_weight,
    blend_weight,
    rows_normed,
    head_mask,
    queries,
    keys,
    values_t,
    slots,
    asked,
    parts,
    back,
    logs,
    back_logs,
    ids_square,
    span_row,
    span_smem,
    local_row,
    table,
    table_smem,
    gated,
    spatial,
    blend,
    moments,
    other_moments,
    mixed,
    other_mixed,
    load_tokens,
    load_store,
    load_small,
    send_query,
    recv_query,
    send_table,
    recv_table,
    send_part,
    recv_part,
    send_log,
    recv_log,
    send_moments,
    recv_moments,
    send_mixed,
    recv_mixed,
    span_sem,
    table_sem,
):
    me = lax.axis_index("st")
    core = lax.axis_index("tp")
    pick_count, span_count = ids_ref.shape
    span_length, width = slots.shape[1:]
    passage_count, passage_length = keys.shape[:2]
    heads, block_length = position_bias.shape
    head_dim = width // heads
    row_count = tokens.shape[0]
    half = row_count // 2
    my_z, my_y, my_x = lax.div(me, SIDE * SIDE), lax.rem(lax.div(me, SIDE), SIDE), lax.rem(me, SIDE)
    ahead = [
        [lax.rem(digit + d, SIDE) * unit for d in range(SIDE)]
        for digit, unit in ((my_z, SIDE * SIDE), (my_y, SIDE), (my_x, 1))
    ]
    peers = [ahead[0][dz] + ahead[1][dy] + ahead[2][dx] for dz, dy, dx in OFFSETS]

    def sources(group):
        a, b = lax.div(group, SIDE), lax.rem(group, SIDE)
        return [
            lax.rem(my_z - b - j + 2 * SIDE, SIDE) * (SIDE * SIDE)
            + lax.rem(my_y - a - j + 2 * SIDE, SIDE) * SIDE
            + lax.rem(my_x - j + SIDE, SIDE)
            for j in range(GROUP)
        ]

    barrier = pltpu.get_barrier_semaphore()
    for peer in peers[1:]:
        pl.semaphore_signal(barrier, inc=1, device_id=(peer, core), device_id_type=MESH)
    pl.semaphore_signal(barrier, inc=1, device_id=(me, 1 - core), device_id_type=MESH)

    def tile_rows(i, size):
        return pl.ds(pl.multiple_of(i * size, size), size)

    def token_load(i):
        rows = tile_rows(i, TILE)
        return pltpu.make_async_copy(tokens_hbm.at[rows], tokens.at[rows], load_tokens.at[i])

    def store_load(i):
        rows = tile_rows(i, TILE)
        return pltpu.make_async_copy(store_hbm.at[rows], store.at[rows], load_store.at[i])

    small = {}
    for n, (name, source, target) in enumerate(
        (
            ("token_gain", token_gain_hbm, token_gain),
            ("query_weight", query_weight_hbm, query_weight),
            ("store_gain", store_gain_hbm, store_gain),
            ("key_weight", key_weight_hbm, key_weight),
            ("read_weight", read_weight_hbm, read_weight),
            ("spatial_weight", spatial_weight_hbm, spatial_weight),
            ("spatial_gain", spatial_gain_hbm, spatial_gain),
            ("carry_weight", carry_weight_hbm, carry_weight),
            ("blend_weight", blend_weight_hbm, blend_weight),
            ("position_mix", position_mix_hbm, position_mix),
            ("position_bias", position_bias_hbm, position_bias),
        )
    ):
        small[name] = pltpu.make_async_copy(source, target, load_small.at[n])
    small["token_gain"].start()
    token_tiles = row_count // TILE
    store_tiles = store.shape[0] // TILE
    for i in range(token_tiles):
        token_load(i).start()
    small["query_weight"].start()
    small["store_gain"].start()
    small["key_weight"].start()
    small["read_weight"].start()
    for i in range(store_tiles):
        store_load(i).start()
    for name in (
        "spatial_weight",
        "spatial_gain",
        "carry_weight",
        "blend_weight",
        "position_mix",
        "position_bias",
    ):
        small[name].start()

    ids_square[...] = jnp.zeros_like(ids_square)
    ids_square[:pick_count, :span_count] = ids_ref[...].astype(jnp.float32)
    ids = ids_square[...].T[:span_count].astype(jnp.int32)
    lane = lax.broadcasted_iota(jnp.int32, (span_count, 128), 1) * passage_count
    span_index = lax.broadcasted_iota(jnp.int32, (span_count, 128), 0)
    slot_span = jnp.zeros((span_count, 128), jnp.int32)
    slot_local = jnp.zeros((span_count, 128), jnp.int32)
    for k in range(pick_count):
        local = ids[:, k : k + 1] - lane
        hit = (local >= 0) & (local < passage_count)
        slot_span = slot_span + jnp.where(hit, span_index, 0)
        slot_local = slot_local + jnp.where(hit, local, 0)
    slot_span = jnp.sum(slot_span, axis=0, keepdims=True)
    slot_local = jnp.sum(slot_local, axis=0, keepdims=True)
    span_row[...] = jnp.minimum(slot_span, span_count - 1)
    local_row[...] = jnp.minimum(slot_local, passage_count - 1)
    table[me] = local_row[...]
    mask_lane = lax.broadcasted_iota(jnp.int32, (span_length, width), 1) // head_dim
    for h in range(heads):
        head_mask[h] = jnp.where(mask_lane == h, 1.0, 0.0).astype(jnp.bfloat16)
    span_copy = pltpu.make_async_copy(span_row, span_smem, span_sem)
    span_copy.start()

    small["token_gain"].wait()

    def token_query(i):
        found = jnp.dot(
            tokens[i * TILE : (i + 1) * TILE, :], query_weight[...], preferred_element_type=jnp.float32
        ).astype(jnp.bfloat16)
        spans = TILE // span_length
        for s in range(spans):
            queries[i * spans + s] = found[s * span_length : (s + 1) * span_length]

    for i in range(token_tiles):
        token_load(i).wait()
        if i == 1:
            small["query_weight"].wait()
        norm_rows(tokens, tokens, token_gain, TILE, i * TILE, i * TILE, TILE // CHUNK if i else 4)
        if i:
            token_query(i - 1)
    token_query(token_tiles - 1)
    span_copy.wait()

    def fill(slot, carry):
        slots[slot] = queries[span_smem[0, slot]]
        return carry

    lax.fori_loop(0, N_ST, fill, 0, unroll=4)
    pl.semaphore_wait(barrier, N_ST)

    def table_copy(peer):
        return pltpu.make_async_remote_copy(
            src_ref=local_row,
            dst_ref=table.at[me],
            send_sem=send_table,
            recv_sem=recv_table,
            device_id=(peer, core),
            device_id_type=MESH,
        )

    def query_copy(peer):
        return pltpu.make_async_remote_copy(
            src_ref=slots.at[peer],
            dst_ref=asked.at[me],
            send_sem=send_query,
            recv_sem=recv_query.at[me],
            device_id=(peer, core),
            device_id_type=MESH,
        )

    for peer in peers[1:]:
        table_copy(peer).start()
    for peer in peers[1:]:
        query_copy(peer).start()
    asked[me] = slots[me]

    small["store_gain"].wait()
    small["key_weight"].wait()
    small["read_weight"].wait()

    def project(i, carry):
        store_load(i).wait()
        norm_rows(store, rows_normed, store_gain, TILE, i * TILE, 0)
        rows = rows_normed[...]
        key_rows = jnp.dot(rows, key_weight[...], preferred_element_type=jnp.float32)
        value_rows = jnp.dot(rows, read_weight[...], preferred_element_type=jnp.float32)
        several = TILE // passage_length
        for p in range(several):
            part = slice(p * passage_length, (p + 1) * passage_length)
            keys[i * several + p] = key_rows[part].astype(jnp.bfloat16)
            values_t[i * several + p] = value_rows[part].T.astype(jnp.bfloat16)
        return carry

    lax.fori_loop(0, store_tiles, project, 0)

    rest = pl.ds(0, N_ST - 1)
    pltpu.make_async_copy(table.at[rest], table.at[rest], recv_table).wait()
    table_read = pltpu.make_async_copy(table, table_smem, table_sem)
    table_read.start()
    table_read.wait()

    def attend(source):
        index = table_smem[source, 0, me]
        query = asked[source]
        spread = jnp.concatenate([query * head_mask[h] for h in range(heads)], axis=0)
        scores = lax.dot_general(
            keys[index], spread, (((1,), (1,)), ((), ())), preferred_element_type=jnp.float32
        ) * (head_dim**-0.5)
        peak = jnp.max(scores, axis=0, keepdims=True)
        weights = jnp.exp(scores - peak)
        total = jnp.sum(weights, axis=0, keepdims=True)
        summed = jnp.dot(
            values_t[index], weights.astype(jnp.bfloat16), preferred_element_type=jnp.float32
        )
        mine = summed[:head_dim]
        for h in range(1, heads):
            mine = jnp.where(mask_lane == h, summed[h * head_dim : (h + 1) * head_dim], mine)
        return (mine / total).astype(jnp.bfloat16), peak + jnp.log(total)

    def part_copy(source):
        return pltpu.make_async_remote_copy(
            src_ref=parts.at[source],
            dst_ref=back.at[me],
            send_sem=send_part,
            recv_sem=recv_part,
            device_id=(source, core),
            device_id_type=MESH,
        )

    def log_copy(source):
        return pltpu.make_async_remote_copy(
            src_ref=logs.at[source],
            dst_ref=back_logs.at[me],
            send_sem=send_log,
            recv_sem=recv_log,
            device_id=(source, core),
            device_id_type=MESH,
        )

    def send_back(source):
        part_copy(source).start()
        log_copy(source).start()

    def serve(group, carry):
        now = sources(group)
        for j, source in enumerate(now):

            @pl.when(group + j > 0)
            def _(source=source):
                pltpu.make_async_copy(asked.at[source], asked.at[source], recv_query.at[source]).wait()

        for source in now:
            part, log_total = attend(source)
            parts[source] = part
            logs[source] = log_total

        for j, source in enumerate(sources(group - 1)):

            @pl.when((group > 1) | ((group == 1) & (j > 0)))
            def _(source=source):
                send_back(source)

        return carry

    lax.fori_loop(0, N_ST // GROUP, serve, 0)
    for source in sources(N_ST // GROUP - 1):
        send_back(source)
    back[me] = parts[me]
    back_logs[me] = logs[me]

    small["spatial_weight"].wait()
    moment_lane = lax.broadcasted_iota(jnp.int32, (TILE, 128), 1)

    def spatial_tile(i, carry):
        rows = tile_rows(i, TILE)
        found = gelu(
            jnp.dot(tokens[rows, :], spatial_weight[...], preferred_element_type=jnp.float32)
        )
        spatial[rows, :] = found
        one = jnp.sum(found, axis=1, keepdims=True)
        two = jnp.sum(found * found, axis=1, keepdims=True)
        moments[rows, :] = jnp.where(moment_lane < 64, one, two)
        return carry

    lax.fori_loop(0, token_tiles, spatial_tile, 0)
    small["carry_weight"].wait()
    small["blend_weight"].wait()

    def carry_tile(i, carry):
        rows = tile_rows(i, TILE)
        gated[rows, :] = gelu(
            jnp.dot(tokens[rows, :], carry_weight[...], preferred_element_type=jnp.float32)
        )
        blend[rows, :] = jax.nn.sigmoid(
            jnp.dot(tokens[rows, :], blend_weight[...], preferred_element_type=jnp.float32)
        )
        return carry

    moment_copy = pltpu.make_async_remote_copy(
        src_ref=moments,
        dst_ref=other_moments,
        send_sem=send_moments,
        recv_sem=recv_moments,
        device_id=(me, 1 - core),
        device_id_type=MESH,
    )
    moment_copy.start()
    lax.fori_loop(0, token_tiles, carry_tile, 0)
    small["spatial_gain"].wait()
    small["position_mix"].wait()
    small["position_bias"].wait()
    moment_copy.wait()
    block_head = lax.broadcasted_iota(jnp.int32, (block_length, width), 1) // head_dim
    bias_columns = jnp.concatenate([position_bias[...]] * (8 // heads), axis=0).T
    bias = jnp.zeros((block_length, width), jnp.float32)
    for h in range(heads):
        bias = jnp.where(block_head == h, bias_columns[:, h : h + 1], bias)

    def mix_block(i, carry):
        rows = tile_rows(i, block_length)
        both = (moments[rows, :] + other_moments[rows, :]) * (0.5 / width)
        mean = both[:, :1]
        spread = both[:, 64:65] - mean * mean
        fed = (
            (spatial[rows, :] - mean) * lax.rsqrt(spread + norm_eps) * spatial_gain[...]
        ).astype(jnp.bfloat16)
        every = jnp.dot(position_mix[...], fed, preferred_element_type=jnp.float32)
        found = every[:block_length]
        for h in range(1, heads):
            found = jnp.where(
                block_head == h, every[h * block_length : (h + 1) * block_length], found
            )
        gated[rows, :] = gated[rows, :] * (found + bias)
        return carry

    lax.fori_loop(0, row_count // block_length, mix_block, 0)

    pltpu.make_async_copy(back.at[rest], back.at[rest], recv_part).wait()
    pltpu.make_async_copy(back_logs.at[rest], back_logs.at[rest], recv_log).wait()

    def merge(span):
        owners = [lax.div(ids_smem[k, span], passage_count) for k in range(pick_count)]
        levels = [back_logs[o] for o in owners]
        top = functools.reduce(jnp.maximum, levels)
        scales = [jnp.exp(level - top) for level in levels]
        total = functools.reduce(jnp.add, scales)
        summed = functools.reduce(
            jnp.add, [s * back[o].astype(jnp.float32) for s, o in zip(scales, owners)]
        )
        turned = (summed / total).T
        memory = jnp.concatenate(
            [turned[h * span_length : (h + 1) * span_length] for h in range(heads)], axis=1
        )
        rows = tile_rows(span, span_length)
        mixed[rows, :] = (gated[rows, :] + blend[rows, :] * memory).astype(jnp.bfloat16)

    def merge_half(first):
        def some(i, carry):
            merge(first + 2 * i)
            merge(first + 2 * i + 1)
            return carry

        lax.fori_loop(0, span_count // 4, some, 0)

    merge_half((1 - core) * (span_count // 2))
    mixed_copy = pltpu.make_async_remote_copy(
        src_ref=mixed.at[tile_rows(1 - core, half)],
        dst_ref=other_mixed,
        send_sem=send_mixed,
        recv_sem=recv_mixed,
        device_id=(me, 1 - core),
        device_id_type=MESH,
    )
    mixed_copy.start()
    merge_half(core * (span_count // 2))
    mine = tile_rows(core, half)

    @pl.when(core == 0)
    def _():
        out_ref[:, :width] = mixed[mine, :]

    @pl.when(core == 1)
    def _():
        out_ref[:, width:] = mixed[mine, :]

    mixed_copy.wait()

    @pl.when(core == 0)
    def _():
        out_ref[:, width:] = other_mixed[...]

    @pl.when(core == 1)
    def _():
        out_ref[:, :width] = other_mixed[...]

    pltpu.make_async_copy(slots.at[rest], slots.at[rest], send_query).wait()
    pltpu.make_async_copy(table.at[rest], table.at[rest], send_table).wait()
    pltpu.make_async_copy(parts.at[rest], parts.at[rest], send_part).wait()
    pltpu.make_async_copy(logs.at[rest], logs.at[rest], send_log).wait()


def per_device(
    tokens,
    route_ids,
    store,
    token_gain,
    store_gain,
    carry_weight,
    spatial_weight,
    spatial_gain,
    position_mix,
    position_bias,
    query_weight,
    key_weight,
    read_weight,
    blend_weight,
    output_weight,
):
    row_count, features = tokens.shape
    heads, block_length = position_mix.shape[:2]
    width = carry_weight.shape[1]
    span_count = route_ids.shape[0]
    span_length = row_count // span_count
    passage_count, passage_length = store.shape[:2]
    store = store.reshape(passage_count * passage_length, features)
    token_gain = token_gain.reshape(1, features)
    store_gain = store_gain.reshape(1, features)
    spatial_gain = spatial_gain.reshape(1, width)
    position_mix = position_mix.reshape(heads * block_length, block_length)
    bf16, f32 = jnp.bfloat16, jnp.float32
    block = pltpu.VMEM((N_ST, span_length, width), bf16)
    weight = pltpu.VMEM((features, width), bf16)
    by_row = pltpu.VMEM((row_count, width), f32)
    dma = pltpu.SemaphoreType.DMA
    anywhere = pl.BlockSpec(memory_space=pl.ANY)
    by_rows = pl.pallas_call(
        layer_kernel,
        out_shape=jax.ShapeDtypeStruct((row_count // 2, 2 * width), bf16),
        in_specs=[
            pl.BlockSpec(memory_space=pltpu.SMEM),
            pl.BlockSpec(memory_space=pltpu.VMEM),
        ]
        + [anywhere] * 13,
        out_specs=pl.BlockSpec(memory_space=pltpu.VMEM),
        scratch_shapes=[
            pltpu.VMEM(tokens.shape, bf16),
            pltpu.VMEM(store.shape, bf16),
            pltpu.VMEM((1, features), f32),
            pltpu.VMEM((1, features), f32),
            weight,
            weight,
            pltpu.VMEM((1, width), f32),
            pltpu.VMEM(position_mix.shape, bf16),
            pltpu.VMEM(position_bias.shape, f32),
            weight,
            weight,
            weight,
            weight,
            pltpu.VMEM((TILE, features), bf16),
            pltpu.VMEM((heads, span_length, width), bf16),
            pltpu.VMEM((span_count, span_length, width), bf16),
            pltpu.VMEM((passage_count, passage_length, width), bf16),
            pltpu.VMEM((passage_count, width, passage_length), bf16),
            block,
            block,
            block,
            block,
            pltpu.VMEM((N_ST, 1, width), f32),
            pltpu.VMEM((N_ST, 1, width), f32),
            pltpu.VMEM((8, 128), f32),
            pltpu.VMEM((1, 128), jnp.int32),
            pltpu.SMEM((1, 128), jnp.int32),
            pltpu.VMEM((1, 128), jnp.int32),
            pltpu.VMEM((N_ST, 1, 128), jnp.int32),
            pltpu.SMEM((N_ST, 1, 128), jnp.int32),
            by_row,
            by_row,
            by_row,
            pltpu.VMEM((row_count, 128), f32),
            pltpu.VMEM((row_count, 128), f32),
            pltpu.VMEM((row_count, width), bf16),
            pltpu.VMEM((row_count // 2, width), bf16),
            dma((row_count // TILE,)),
            dma((store.shape[0] // TILE,)),
            dma((11,)),
            dma,
            dma((N_ST,)),
        ]
        + [dma] * 12,
        compiler_params=pltpu.CompilerParams(
            collective_id=0, has_side_effects=True, vmem_limit_bytes=60 << 20
        ),
    )(
        route_ids.T,
        route_ids.T,
        tokens,
        store,
        token_gain,
        store_gain,
        carry_weight,
        spatial_weight,
        spatial_gain,
        position_mix,
        position_bias,
        query_weight,
        key_weight,
        read_weight,
        blend_weight,
    )
    return jnp.dot(by_rows, output_weight, preferred_element_type=f32).astype(bf16)


def solution(mesh):
    in_specs = (
        P("st", None),
        P("st", None),
        P("st", None, None),
        P(),
        P(),
        P(None, "tp"),
        P(None, "tp"),
        P("tp"),
        P("tp", None, None),
        P("tp", None),
        P(None, "tp"),
        P(None, "tp"),
        P(None, "tp"),
        P(None, "tp"),
        P(),
    )
    out_specs = P(("st", "tp"), None)
    return jax.shard_map(
        per_device, mesh=mesh, in_specs=in_specs, out_specs=out_specs, check_vma=False
    )
```

```python
import functools

import jax
import jax.numpy as jnp
from jax import lax
from jax.experimental import pallas as pl
from jax.experimental.pallas import tpu as pltpu
from jax.sharding import PartitionSpec as P

norm_eps = 1e-06
MESH = pl.DeviceIdType.MESH
SIDE = 4
N_ST = SIDE**3
GROUP = 4
CHUNK = 16
TILE = 256


OFFSETS = [
    ((b + j) % SIDE, (a + j) % SIDE, j)
    for a in range(SIDE)
    for b in range(SIDE)
    for j in range(SIDE)
]


def gelu(x):
    return 0.5 * x * (1.0 + lax.erf(x * 0.5**0.5))


def norm_rows(source, target, gain_ref, count, source_base, target_base, unroll=4):
    features = source.shape[1]
    gain = gain_ref[...]

    def some(i, carry):
        rows = pl.ds(pl.multiple_of(source_base + i * CHUNK, CHUNK), CHUNK)
        values = source[rows, :].astype(jnp.float32)
        mean = jnp.sum(values * values, axis=1, keepdims=True) * (1.0 / features)
        scaled = values * lax.rsqrt(mean + norm_eps) * gain
        rows = pl.ds(pl.multiple_of(target_base + i * CHUNK, CHUNK), CHUNK)
        target[rows, :] = scaled.astype(jnp.bfloat16)
        return carry

    lax.fori_loop(0, count // CHUNK, some, 0, unroll=unroll)


def layer_kernel(
    ids_smem,
    ids_ref,
    tokens_hbm,
    store_hbm,
    token_gain_hbm,
    store_gain_hbm,
    carry_weight_hbm,
    spatial_weight_hbm,
    spatial_gain_hbm,
    position_mix_hbm,
    position_bias_hbm,
    query_weight_hbm,
    key_weight_hbm,
    read_weight_hbm,
    blend_weight_hbm,
    out_ref,
    tokens,
    store,
    token_gain,
    store_gain,
    carry_weight,
    spatial_weight,
    spatial_gain,
    position_mix,
    position_bias,
    query_weight,
    key_weight,
    read_weight,
    blend_weight,
    rows_normed,
    head_mask,
    queries,
    keys,
    values_t,
    slots,
    asked,
    parts,
    back,
    logs,
    back_logs,
    ids_square,
    span_row,
    span_smem,
    local_row,
    table,
    table_smem,
    gated,
    spatial,
    blend,
    moments,
    other_moments,
    mixed,
    load_tokens,
    load_store,
    load_small,
    send_query,
    recv_query,
    send_table,
    recv_table,
    send_part,
    recv_part,
    send_log,
    recv_log,
    send_moments,
    recv_moments,
    send_mixed,
    recv_mixed,
    span_sem,
    table_sem,
):
    me = lax.axis_index("st")
    core = lax.axis_index("tp")
    pick_count, span_count = ids_ref.shape
    span_length, width = slots.shape[1:]
    passage_count, passage_length = keys.shape[:2]
    heads, block_length = position_bias.shape
    head_dim = width // heads
    row_count = tokens.shape[0]
    my_z, my_y, my_x = lax.div(me, SIDE * SIDE), lax.rem(lax.div(me, SIDE), SIDE), lax.rem(me, SIDE)
    ahead = [
        [lax.rem(digit + d, SIDE) * unit for d in range(SIDE)]
        for digit, unit in ((my_z, SIDE * SIDE), (my_y, SIDE), (my_x, 1))
    ]
    peers = [ahead[0][dz] + ahead[1][dy] + ahead[2][dx] for dz, dy, dx in OFFSETS]

    def sources(group):
        a, b = lax.div(group, SIDE), lax.rem(group, SIDE)
        return [
            lax.rem(my_z - b - j + 2 * SIDE, SIDE) * (SIDE * SIDE)
            + lax.rem(my_y - a - j + 2 * SIDE, SIDE) * SIDE
            + lax.rem(my_x - j + SIDE, SIDE)
            for j in range(GROUP)
        ]

    barrier = pltpu.get_barrier_semaphore()
    for peer in peers[1:]:
        pl.semaphore_signal(barrier, inc=1, device_id=(peer, core), device_id_type=MESH)
    pl.semaphore_signal(barrier, inc=1, device_id=(me, 1 - core), device_id_type=MESH)

    def tile_rows(i, size):
        return pl.ds(pl.multiple_of(i * size, size), size)

    def token_load(i):
        rows = tile_rows(i, TILE)
        return pltpu.make_async_copy(tokens_hbm.at[rows], tokens.at[rows], load_tokens.at[i])

    def store_load(i):
        rows = tile_rows(i, TILE)
        return pltpu.make_async_copy(store_hbm.at[rows], store.at[rows], load_store.at[i])

    small = {}
    for n, (name, source, target) in enumerate(
        (
            ("token_gain", token_gain_hbm, token_gain),
            ("query_weight", query_weight_hbm, query_weight),
            ("store_gain", store_gain_hbm, store_gain),
            ("key_weight", key_weight_hbm, key_weight),
            ("read_weight", read_weight_hbm, read_weight),
            ("spatial_weight", spatial_weight_hbm, spatial_weight),
            ("spatial_gain", spatial_gain_hbm, spatial_gain),
            ("carry_weight", carry_weight_hbm, carry_weight),
            ("blend_weight", blend_weight_hbm, blend_weight),
            ("position_mix", position_mix_hbm, position_mix),
            ("position_bias", position_bias_hbm, position_bias),
        )
    ):
        small[name] = pltpu.make_async_copy(source, target, load_small.at[n])
    small["token_gain"].start()
    token_tiles = row_count // TILE
    store_tiles = store.shape[0] // TILE
    for i in range(token_tiles):
        token_load(i).start()
    small["query_weight"].start()

    def start_later_loads():
        small["store_gain"].start()
        small["key_weight"].start()
        small["read_weight"].start()
        for i in range(store_tiles):
            store_load(i).start()
        for name in (
            "spatial_weight",
            "spatial_gain",
            "carry_weight",
            "blend_weight",
            "position_mix",
            "position_bias",
        ):
            small[name].start()

    ids_square[...] = jnp.zeros_like(ids_square)
    ids_square[:pick_count, :span_count] = ids_ref[...].astype(jnp.float32)
    ids = ids_square[...].T[:span_count].astype(jnp.int32)
    lane = lax.broadcasted_iota(jnp.int32, (span_count, 128), 1) * passage_count
    span_index = lax.broadcasted_iota(jnp.int32, (span_count, 128), 0)
    slot_span = jnp.zeros((span_count, 128), jnp.int32)
    slot_local = jnp.zeros((span_count, 128), jnp.int32)
    for k in range(pick_count):
        local = ids[:, k : k + 1] - lane
        hit = (local >= 0) & (local < passage_count)
        slot_span = slot_span + jnp.where(hit, span_index, 0)
        slot_local = slot_local + jnp.where(hit, local, 0)
    slot_span = jnp.sum(slot_span, axis=0, keepdims=True)
    slot_local = jnp.sum(slot_local, axis=0, keepdims=True)
    span_row[...] = jnp.minimum(slot_span, span_count - 1)
    local_row[...] = jnp.minimum(slot_local, passage_count - 1)
    table[me] = local_row[...]
    mask_lane = lax.broadcasted_iota(jnp.int32, (span_length, width), 1) // head_dim
    for h in range(heads):
        head_mask[h] = jnp.where(mask_lane == h, 1.0, 0.0).astype(jnp.bfloat16)
    span_copy = pltpu.make_async_copy(span_row, span_smem, span_sem)
    span_copy.start()

    small["token_gain"].wait()

    def token_query(i):
        found = jnp.dot(
            tokens[i * TILE : (i + 1) * TILE, :], query_weight[...], preferred_element_type=jnp.float32
        ).astype(jnp.bfloat16)
        spans = TILE // span_length
        for s in range(spans):
            queries[i * spans + s] = found[s * span_length : (s + 1) * span_length]

    for i in range(token_tiles):
        token_load(i).wait()
        if i == token_tiles - 1:
            small["query_weight"].wait()
            start_later_loads()
        norm_rows(tokens, tokens, token_gain, TILE, i * TILE, i * TILE, TILE // CHUNK if i == token_tiles - 1 else 4)
        if i == token_tiles - 1:
            for k in range(i):
                token_query(k)
    token_query(token_tiles - 1)
    span_copy.wait()

    def fill(slot, carry):
        slots[slot] = queries[span_smem[0, slot]]
        return carry

    lax.fori_loop(0, N_ST, fill, 0, unroll=4)
    pl.semaphore_wait(barrier, N_ST)

    def table_copy(peer):
        return pltpu.make_async_remote_copy(
            src_ref=local_row,
            dst_ref=table.at[me],
            send_sem=send_table,
            recv_sem=recv_table,
            device_id=(peer, core),
            device_id_type=MESH,
        )

    def query_copy(peer):
        return pltpu.make_async_remote_copy(
            src_ref=slots.at[peer],
            dst_ref=asked.at[me],
            send_sem=send_query,
            recv_sem=recv_query.at[me],
            device_id=(peer, core),
            device_id_type=MESH,
        )

    for peer in peers[1:]:
        table_copy(peer).start()
    for peer in peers[1:]:
        query_copy(peer).start()
    asked[me] = slots[me]

    small["store_gain"].wait()
    small["key_weight"].wait()
    small["read_weight"].wait()

    def project(i, carry):
        store_load(i).wait()
        norm_rows(store, rows_normed, store_gain, TILE, i * TILE, 0)
        rows = rows_normed[...]
        key_rows = jnp.dot(rows, key_weight[...], preferred_element_type=jnp.float32)
        value_rows = jnp.dot(rows, read_weight[...], preferred_element_type=jnp.float32)
        several = TILE // passage_length
        for p in range(several):
            part = slice(p * passage_length, (p + 1) * passage_length)
            keys[i * several + p] = key_rows[part].astype(jnp.bfloat16)
            values_t[i * several + p] = value_rows[part].T.astype(jnp.bfloat16)
        return carry

    lax.fori_loop(0, store_tiles, project, 0)

    rest = pl.ds(0, N_ST - 1)
    pltpu.make_async_copy(table.at[rest], table.at[rest], recv_table).wait()
    table_read = pltpu.make_async_copy(table, table_smem, table_sem)
    table_read.start()
    table_read.wait()

    def attend(source):
        index = table_smem[source, 0, me]
        query = asked[source]
        spread = jnp.concatenate([query * head_mask[h] for h in range(heads)], axis=0)
        scores = lax.dot_general(
            keys[index], spread, (((1,), (1,)), ((), ())), preferred_element_type=jnp.float32
        ) * (head_dim**-0.5)
        peak = jnp.max(scores, axis=0, keepdims=True)
        weights = jnp.exp(scores - peak)
        total = jnp.sum(weights, axis=0, keepdims=True)
        summed = jnp.dot(
            values_t[index], weights.astype(jnp.bfloat16), preferred_element_type=jnp.float32
        )
        mine = summed[:head_dim]
        for h in range(1, heads):
            mine = jnp.where(mask_lane == h, summed[h * head_dim : (h + 1) * head_dim], mine)
        return (mine / total).astype(jnp.bfloat16), peak + jnp.log(total)

    def part_copy(source):
        return pltpu.make_async_remote_copy(
            src_ref=parts.at[source],
            dst_ref=back.at[me],
            send_sem=send_part,
            recv_sem=recv_part,
            device_id=(source, core),
            device_id_type=MESH,
        )

    def log_copy(source):
        return pltpu.make_async_remote_copy(
            src_ref=logs.at[source],
            dst_ref=back_logs.at[me],
            send_sem=send_log,
            recv_sem=recv_log,
            device_id=(source, core),
            device_id_type=MESH,
        )

    def send_back(source):
        part_copy(source).start()
        log_copy(source).start()

    def serve(group, carry):
        now = sources(group)
        for j, source in enumerate(now):

            @pl.when(group + j > 0)
            def _(source=source):
                pltpu.make_async_copy(asked.at[source], asked.at[source], recv_query.at[source]).wait()

        for source in now:
            part, log_total = attend(source)
            parts[source] = part
            logs[source] = log_total

        for j, source in enumerate(sources(group - 1)):

            @pl.when((group > 1) | ((group == 1) & (j > 0)))
            def _(source=source):
                send_back(source)

        return carry

    lax.fori_loop(0, N_ST // GROUP, serve, 0)
    for source in sources(N_ST // GROUP - 1):
        send_back(source)
    back[me] = parts[me]
    back_logs[me] = logs[me]

    small["spatial_weight"].wait()
    moment_lane = lax.broadcasted_iota(jnp.int32, (TILE, 128), 1)

    def spatial_tile(i, carry):
        rows = tile_rows(i, TILE)
        found = gelu(
            jnp.dot(tokens[rows, :], spatial_weight[...], preferred_element_type=jnp.float32)
        )
        spatial[rows, :] = found
        one = jnp.sum(found, axis=1, keepdims=True)
        two = jnp.sum(found * found, axis=1, keepdims=True)
        moments[rows, :] = jnp.where(moment_lane < 64, one, two)
        return carry

    lax.fori_loop(0, token_tiles, spatial_tile, 0)
    small["carry_weight"].wait()
    small["blend_weight"].wait()

    def carry_tile(i, carry):
        rows = tile_rows(i, TILE)
        gated[rows, :] = gelu(
            jnp.dot(tokens[rows, :], carry_weight[...], preferred_element_type=jnp.float32)
        )
        blend[rows, :] = jax.nn.sigmoid(
            jnp.dot(tokens[rows, :], blend_weight[...], preferred_element_type=jnp.float32)
        )
        return carry

    moment_copy = pltpu.make_async_remote_copy(
        src_ref=moments,
        dst_ref=other_moments,
        send_sem=send_moments,
        recv_sem=recv_moments,
        device_id=(me, 1 - core),
        device_id_type=MESH,
    )
    moment_copy.start()
    lax.fori_loop(0, token_tiles, carry_tile, 0)
    small["spatial_gain"].wait()
    small["position_mix"].wait()
    small["position_bias"].wait()
    moment_copy.wait()
    block_head = lax.broadcasted_iota(jnp.int32, (block_length, width), 1) // head_dim
    bias_columns = jnp.concatenate([position_bias[...]] * (8 // heads), axis=0).T
    bias = jnp.zeros((block_length, width), jnp.float32)
    for h in range(heads):
        bias = jnp.where(block_head == h, bias_columns[:, h : h + 1], bias)

    def mix_block(i, carry):
        rows = tile_rows(i, block_length)
        both = (moments[rows, :] + other_moments[rows, :]) * (0.5 / width)
        mean = both[:, :1]
        spread = both[:, 64:65] - mean * mean
        fed = (
            (spatial[rows, :] - mean) * lax.rsqrt(spread + norm_eps) * spatial_gain[...]
        ).astype(jnp.bfloat16)
        every = jnp.dot(position_mix[...], fed, preferred_element_type=jnp.float32)
        found = every[:block_length]
        for h in range(1, heads):
            found = jnp.where(
                block_head == h, every[h * block_length : (h + 1) * block_length], found
            )
        gated[rows, :] = gated[rows, :] * (found + bias)
        return carry

    lax.fori_loop(0, row_count // block_length, mix_block, 0)

    pltpu.make_async_copy(back.at[rest], back.at[rest], recv_part).wait()
    pltpu.make_async_copy(back_logs.at[rest], back_logs.at[rest], recv_log).wait()

    def merge(span):
        owners = [lax.div(ids_smem[k, span], passage_count) for k in range(pick_count)]
        levels = [back_logs[o] for o in owners]
        top = functools.reduce(jnp.maximum, levels)
        scales = [jnp.exp(level - top) for level in levels]
        total = functools.reduce(jnp.add, scales)
        summed = functools.reduce(
            jnp.add, [s * back[o].astype(jnp.float32) for s, o in zip(scales, owners)]
        )
        turned = (summed / total).T
        memory = jnp.concatenate(
            [turned[h * span_length : (h + 1) * span_length] for h in range(heads)], axis=1
        )
        rows = tile_rows(span, span_length)
        return (gated[rows, :] + blend[rows, :] * memory).astype(jnp.bfloat16)

    columns = pl.ds(pl.multiple_of(core * width, width), width)
    half_spans = span_count // 2
    pieces = send_mixed.shape[0]
    per_piece = half_spans // pieces

    def mixed_copy(i):
        rows = tile_rows(i, per_piece * span_length)
        return pltpu.make_async_remote_copy(
            src_ref=mixed.at[rows],
            dst_ref=out_ref.at[rows, columns],
            send_sem=send_mixed.at[i],
            recv_sem=recv_mixed.at[i],
            device_id=(me, 1 - core),
            device_id_type=MESH,
        )

    def merge_theirs(i, carry):
        for k in range(per_piece):
            span = i * per_piece + k
            mixed[tile_rows(span, span_length), :] = merge((1 - core) * half_spans + span)

        @pl.when(i > 0)
        def _():
            mixed_copy(i - 1).start()

        return carry

    lax.fori_loop(0, pieces, merge_theirs, 0)
    mixed_copy(pieces - 1).start()

    def merge_mine(i, carry):
        for k in range(per_piece):
            span = i * per_piece + k
            out_ref[tile_rows(span, span_length), columns] = merge(core * half_spans + span)
        return carry

    lax.fori_loop(0, pieces, merge_mine, 0)
    for i in range(pieces):
        mixed_copy(i).wait()
    pltpu.make_async_copy(slots.at[rest], slots.at[rest], send_query).wait()
    pltpu.make_async_copy(table.at[rest], table.at[rest], send_table).wait()
    pltpu.make_async_copy(parts.at[rest], parts.at[rest], send_part).wait()
    pltpu.make_async_copy(logs.at[rest], logs.at[rest], send_log).wait()


def per_device(
    tokens,
    route_ids,
    store,
    token_gain,
    store_gain,
    carry_weight,
    spatial_weight,
    spatial_gain,
    position_mix,
    position_bias,
    query_weight,
    key_weight,
    read_weight,
    blend_weight,
    output_weight,
):
    row_count, features = tokens.shape
    heads, block_length = position_mix.shape[:2]
    width = carry_weight.shape[1]
    span_count = route_ids.shape[0]
    span_length = row_count // span_count
    passage_count, passage_length = store.shape[:2]
    store = store.reshape(passage_count * passage_length, features)
    token_gain = token_gain.reshape(1, features)
    store_gain = store_gain.reshape(1, features)
    spatial_gain = spatial_gain.reshape(1, width)
    position_mix = position_mix.reshape(heads * block_length, block_length)
    bf16, f32 = jnp.bfloat16, jnp.float32
    block = pltpu.VMEM((N_ST, span_length, width), bf16)
    weight = pltpu.VMEM((features, width), bf16)
    by_row = pltpu.VMEM((row_count, width), f32)
    dma = pltpu.SemaphoreType.DMA
    anywhere = pl.BlockSpec(memory_space=pl.ANY)
    by_rows = pl.pallas_call(
        layer_kernel,
        out_shape=pltpu.VMEM((row_count // 2, 2 * width), bf16),
        in_specs=[
            pl.BlockSpec(memory_space=pltpu.SMEM),
            pl.BlockSpec(memory_space=pltpu.VMEM),
        ]
        + [anywhere] * 13,
        out_specs=pl.BlockSpec(memory_space=pltpu.VMEM),
        scratch_shapes=[
            pltpu.VMEM(tokens.shape, bf16),
            pltpu.VMEM(store.shape, bf16),
            pltpu.VMEM((1, features), f32),
            pltpu.VMEM((1, features), f32),
            weight,
            weight,
            pltpu.VMEM((1, width), f32),
            pltpu.VMEM(position_mix.shape, bf16),
            pltpu.VMEM(position_bias.shape, f32),
            weight,
            weight,
            weight,
            weight,
            pltpu.VMEM((TILE, features), bf16),
            pltpu.VMEM((heads, span_length, width), bf16),
            pltpu.VMEM((span_count, span_length, width), bf16),
            pltpu.VMEM((passage_count, passage_length, width), bf16),
            pltpu.VMEM((passage_count, width, passage_length), bf16),
            block,
            block,
            block,
            block,
            pltpu.VMEM((N_ST, 1, width), f32),
            pltpu.VMEM((N_ST, 1, width), f32),
            pltpu.VMEM((8, 128), f32),
            pltpu.VMEM((1, 128), jnp.int32),
            pltpu.SMEM((1, 128), jnp.int32),
            pltpu.VMEM((1, 128), jnp.int32),
            pltpu.VMEM((N_ST, 1, 128), jnp.int32),
            pltpu.SMEM((N_ST, 1, 128), jnp.int32),
            by_row,
            by_row,
            by_row,
            pltpu.VMEM((row_count, 128), f32),
            pltpu.VMEM((row_count, 128), f32),
            pltpu.VMEM((row_count // 2, width), bf16),
            dma((row_count // TILE,)),
            dma((store.shape[0] // TILE,)),
            dma((11,)),
            dma,
            dma((N_ST,)),
        ]
        + [dma] * 8
        + [dma((3,))] * 2
        + [dma] * 2,
        compiler_params=pltpu.CompilerParams(
            collective_id=0, has_side_effects=True, vmem_limit_bytes=60 << 20
        ),
    )(
        route_ids.T,
        route_ids.T,
        tokens,
        store,
        token_gain,
        store_gain,
        carry_weight,
        spatial_weight,
        spatial_gain,
        position_mix,
        position_bias,
        query_weight,
        key_weight,
        read_weight,
        blend_weight,
    )
    return jnp.dot(by_rows, output_weight, preferred_element_type=f32).astype(bf16)


def solution(mesh):
    in_specs = (
        P("st", None),
        P("st", None),
        P("st", None, None),
        P(),
        P(),
        P(None, "tp"),
        P(None, "tp"),
        P("tp"),
        P("tp", None, None),
        P("tp", None),
        P(None, "tp"),
        P(None, "tp"),
        P(None, "tp"),
        P(None, "tp"),
        P(),
    )
    out_specs = P(("st", "tp"), None)
    return jax.shard_map(
        per_device, mesh=mesh, in_specs=in_specs, out_specs=out_specs, check_vma=False
    )
```

```python
import functools

import jax
import jax.numpy as jnp
from jax import lax
from jax.experimental import pallas as pl
from jax.experimental.pallas import tpu as pltpu
from jax.sharding import PartitionSpec as P

norm_eps = 1e-06
MESH = pl.DeviceIdType.MESH
SIDE = 4
N_ST = SIDE**3
GROUP = 4
CHUNK = 16
TILE = 256
AHEAD = 8


OFFSETS = [
    ((b + j) % SIDE, (a + j) % SIDE, j)
    for a in range(SIDE)
    for b in range(SIDE)
    for j in range(SIDE)
]


def gelu(x):
    return 0.5 * x * (1.0 + lax.erf(x * 0.5**0.5))


def norm_rows(source, target, gain_ref, count, source_base, target_base, unroll=4):
    features = source.shape[1]
    gain = gain_ref[...]

    def some(i, carry):
        rows = pl.ds(pl.multiple_of(source_base + i * CHUNK, CHUNK), CHUNK)
        values = source[rows, :].astype(jnp.float32)
        mean = jnp.sum(values * values, axis=1, keepdims=True) * (1.0 / features)
        scaled = values * lax.rsqrt(mean + norm_eps) * gain
        rows = pl.ds(pl.multiple_of(target_base + i * CHUNK, CHUNK), CHUNK)
        target[rows, :] = scaled.astype(jnp.bfloat16)
        return carry

    lax.fori_loop(0, count // CHUNK, some, 0, unroll=unroll)


def layer_kernel(
    ids_smem,
    ids_ref,
    tokens_hbm,
    store_hbm,
    token_gain_hbm,
    store_gain_hbm,
    carry_weight_hbm,
    spatial_weight_hbm,
    spatial_gain_hbm,
    position_mix_hbm,
    position_bias_hbm,
    query_weight_hbm,
    key_weight_hbm,
    read_weight_hbm,
    blend_weight_hbm,
    output_weight_hbm,
    out_ref,
    tokens,
    store,
    token_gain,
    store_gain,
    carry_weight,
    spatial_weight,
    spatial_gain,
    position_mix,
    position_bias,
    query_weight,
    key_weight,
    read_weight,
    blend_weight,
    output_weight,
    rows_normed,
    head_mask,
    queries,
    keys,
    values_t,
    slots,
    asked,
    parts,
    back,
    logs,
    back_logs,
    ids_square,
    span_row,
    span_smem,
    local_row,
    table,
    table_smem,
    gated,
    spatial,
    blend,
    moments,
    other_moments,
    mixed,
    by_rows,
    load_tokens,
    load_store,
    load_small,
    send_query,
    recv_query,
    send_table,
    recv_table,
    send_part,
    recv_part,
    send_log,
    recv_log,
    send_moments,
    recv_moments,
    send_mixed,
    recv_mixed,
    span_sem,
    table_sem,
):
    me = lax.axis_index("st")
    core = lax.axis_index("tp")
    pick_count, span_count = ids_ref.shape
    span_length, width = slots.shape[1:]
    passage_count, passage_length = keys.shape[:2]
    heads, block_length = position_bias.shape
    head_dim = width // heads
    row_count = tokens.shape[0]
    my_z, my_y, my_x = lax.div(me, SIDE * SIDE), lax.rem(lax.div(me, SIDE), SIDE), lax.rem(me, SIDE)
    ahead = [
        [lax.rem(digit + d, SIDE) * unit for d in range(SIDE)]
        for digit, unit in ((my_z, SIDE * SIDE), (my_y, SIDE), (my_x, 1))
    ]
    peers = [ahead[0][dz] + ahead[1][dy] + ahead[2][dx] for dz, dy, dx in OFFSETS]

    def sources(group):
        a, b = lax.div(group, SIDE), lax.rem(group, SIDE)
        return [
            lax.rem(my_z - b - j + 2 * SIDE, SIDE) * (SIDE * SIDE)
            + lax.rem(my_y - a - j + 2 * SIDE, SIDE) * SIDE
            + lax.rem(my_x - j + SIDE, SIDE)
            for j in range(GROUP)
        ]

    def tile_rows(i, size):
        return pl.ds(pl.multiple_of(i * size, size), size)

    def token_load(i):
        rows = tile_rows(i, TILE)
        return pltpu.make_async_copy(tokens_hbm.at[rows], tokens.at[rows], load_tokens.at[i])

    def store_load(i):
        rows = tile_rows(i, TILE)
        return pltpu.make_async_copy(store_hbm.at[rows], store.at[rows], load_store.at[i])

    small = {}
    for n, (name, source, target) in enumerate(
        (
            ("token_gain", token_gain_hbm, token_gain),
            ("query_weight", query_weight_hbm, query_weight),
            ("store_gain", store_gain_hbm, store_gain),
            ("key_weight", key_weight_hbm, key_weight),
            ("read_weight", read_weight_hbm, read_weight),
            ("spatial_weight", spatial_weight_hbm, spatial_weight),
            ("spatial_gain", spatial_gain_hbm, spatial_gain),
            ("carry_weight", carry_weight_hbm, carry_weight),
            ("blend_weight", blend_weight_hbm, blend_weight),
            ("position_mix", position_mix_hbm, position_mix),
            ("position_bias", position_bias_hbm, position_bias),
            ("output_weight", output_weight_hbm, output_weight),
        )
    ):
        small[name] = pltpu.make_async_copy(source, target, load_small.at[n])
    token_tiles = row_count // TILE
    store_tiles = store.shape[0] // TILE
    token_load(0).start()
    small["token_gain"].start()
    small["query_weight"].start()
    for i in range(1, token_tiles):
        token_load(i).start()
    barrier = pltpu.get_barrier_semaphore()
    for peer in peers[1:]:
        pl.semaphore_signal(barrier, inc=1, device_id=(peer, core), device_id_type=MESH)
    pl.semaphore_signal(barrier, inc=1, device_id=(me, 1 - core), device_id_type=MESH)


    def start_later_loads():
        small["store_gain"].start()
        small["key_weight"].start()
        small["read_weight"].start()
        for i in range(store_tiles):
            store_load(i).start()
        for name in (
            "spatial_weight",
            "spatial_gain",
            "carry_weight",
            "blend_weight",
            "position_mix",
            "position_bias",
            "output_weight",
        ):
            small[name].start()

    ids_square[...] = jnp.zeros_like(ids_square)
    ids_square[:pick_count, :span_count] = ids_ref[...].astype(jnp.float32)
    ids = ids_square[...].T[:span_count].astype(jnp.int32)
    lane = lax.broadcasted_iota(jnp.int32, (span_count, 128), 1) * passage_count
    span_index = lax.broadcasted_iota(jnp.int32, (span_count, 128), 0)
    slot_span = jnp.zeros((span_count, 128), jnp.int32)
    slot_local = jnp.zeros((span_count, 128), jnp.int32)
    for k in range(pick_count):
        local = ids[:, k : k + 1] - lane
        hit = (local >= 0) & (local < passage_count)
        slot_span = slot_span + jnp.where(hit, span_index, 0)
        slot_local = slot_local + jnp.where(hit, local, 0)
    slot_span = jnp.sum(slot_span, axis=0, keepdims=True)
    slot_local = jnp.sum(slot_local, axis=0, keepdims=True)
    span_row[...] = jnp.minimum(slot_span, span_count - 1)
    local_row[...] = jnp.minimum(slot_local, passage_count - 1)
    table[me] = local_row[...]
    mask_lane = lax.broadcasted_iota(jnp.int32, (span_length, width), 1) // head_dim
    for h in range(heads):
        head_mask[h] = jnp.where(mask_lane == h, 1.0, 0.0).astype(jnp.bfloat16)
    span_copy = pltpu.make_async_copy(span_row, span_smem, span_sem)
    span_copy.start()

    small["token_gain"].wait()

    def token_query(i):
        found = jnp.dot(
            tokens[i * TILE : (i + 1) * TILE, :], query_weight[...], preferred_element_type=jnp.float32
        ).astype(jnp.bfloat16)
        spans = TILE // span_length
        for s in range(spans):
            queries[i * spans + s] = found[s * span_length : (s + 1) * span_length]

    for i in range(token_tiles):
        token_load(i).wait()
        if i == 1:
            small["query_weight"].wait()
        if i == token_tiles - 1:
            start_later_loads()
        norm_rows(tokens, tokens, token_gain, TILE, i * TILE, i * TILE, TILE // CHUNK if i else 4)
        if i:
            token_query(i - 1)
    token_query(token_tiles - 1)
    span_copy.wait()

    pl.semaphore_wait(barrier, N_ST)

    def table_copy(peer):
        return pltpu.make_async_remote_copy(
            src_ref=local_row,
            dst_ref=table.at[me],
            send_sem=send_table,
            recv_sem=recv_table,
            device_id=(peer, core),
            device_id_type=MESH,
        )

    def query_copy(peer):
        return pltpu.make_async_remote_copy(
            src_ref=slots.at[peer],
            dst_ref=asked.at[me],
            send_sem=send_query,
            recv_sem=recv_query.at[me],
            device_id=(peer, core),
            device_id_type=MESH,
        )

    for peer in peers[1:]:
        table_copy(peer).start()
    for k, peer in enumerate(peers):
        if k > AHEAD:
            query_copy(peers[k - AHEAD]).start()
        slots[peer] = queries[span_smem[0, peer]]
    for peer in peers[N_ST - AHEAD :]:
        query_copy(peer).start()
    asked[me] = slots[me]

    small["store_gain"].wait()
    small["key_weight"].wait()
    small["read_weight"].wait()

    def project(i, carry):
        store_load(i).wait()
        norm_rows(store, rows_normed, store_gain, TILE, i * TILE, 0)
        rows = rows_normed[...]
        key_rows = jnp.dot(rows, key_weight[...], preferred_element_type=jnp.float32)
        value_rows = jnp.dot(rows, read_weight[...], preferred_element_type=jnp.float32)
        several = TILE // passage_length
        for p in range(several):
            part = slice(p * passage_length, (p + 1) * passage_length)
            keys[i * several + p] = key_rows[part].astype(jnp.bfloat16)
            values_t[i * several + p] = value_rows[part].T.astype(jnp.bfloat16)
        return carry

    lax.fori_loop(0, store_tiles, project, 0)

    rest = pl.ds(0, N_ST - 1)
    pltpu.make_async_copy(table.at[rest], table.at[rest], recv_table).wait()
    table_read = pltpu.make_async_copy(table, table_smem, table_sem)
    table_read.start()
    table_read.wait()

    def attend(source):
        index = table_smem[source, 0, me]
        query = asked[source]
        spread = jnp.concatenate([query * head_mask[h] for h in range(heads)], axis=0)
        scores = lax.dot_general(
            keys[index], spread, (((1,), (1,)), ((), ())), preferred_element_type=jnp.float32
        ) * (head_dim**-0.5)
        peak = jnp.max(scores, axis=0, keepdims=True)
        weights = jnp.exp(scores - peak)
        total = jnp.sum(weights, axis=0, keepdims=True)
        summed = jnp.dot(
            values_t[index], weights.astype(jnp.bfloat16), preferred_element_type=jnp.float32
        )
        mine = summed[:head_dim]
        for h in range(1, heads):
            mine = jnp.where(mask_lane == h, summed[h * head_dim : (h + 1) * head_dim], mine)
        return (mine / total).astype(jnp.bfloat16), peak + jnp.log(total)

    def part_copy(source):
        return pltpu.make_async_remote_copy(
            src_ref=parts.at[source],
            dst_ref=back.at[me],
            send_sem=send_part,
            recv_sem=recv_part,
            device_id=(source, core),
            device_id_type=MESH,
        )

    def log_copy(source):
        return pltpu.make_async_remote_copy(
            src_ref=logs.at[source],
            dst_ref=back_logs.at[me],
            send_sem=send_log,
            recv_sem=recv_log,
            device_id=(source, core),
            device_id_type=MESH,
        )

    def send_back(source):
        part_copy(source).start()
        log_copy(source).start()

    def serve(group, carry):
        now = sources(group)
        for j, source in enumerate(now):

            @pl.when(group + j > 0)
            def _(source=source):
                pltpu.make_async_copy(asked.at[source], asked.at[source], recv_query.at[source]).wait()

        for source in now:
            part, log_total = attend(source)
            parts[source] = part
            logs[source] = log_total

        for j, source in enumerate(sources(group - 1)):

            @pl.when((group > 1) | ((group == 1) & (j > 0)))
            def _(source=source):
                send_back(source)

        return carry

    lax.fori_loop(0, N_ST // GROUP, serve, 0)
    for source in sources(N_ST // GROUP - 1):
        send_back(source)
    back[me] = parts[me]
    back_logs[me] = logs[me]

    small["spatial_weight"].wait()
    moment_lane = lax.broadcasted_iota(jnp.int32, (TILE, 128), 1)

    def spatial_tile(i, carry):
        rows = tile_rows(i, TILE)
        found = gelu(
            jnp.dot(tokens[rows, :], spatial_weight[...], preferred_element_type=jnp.float32)
        )
        spatial[rows, :] = found
        one = jnp.sum(found, axis=1, keepdims=True)
        two = jnp.sum(found * found, axis=1, keepdims=True)
        moments[rows, :] = jnp.where(moment_lane < 64, one, two)
        return carry

    lax.fori_loop(0, token_tiles, spatial_tile, 0)
    small["carry_weight"].wait()
    small["blend_weight"].wait()

    def carry_tile(i, carry):
        rows = tile_rows(i, TILE)
        gated[rows, :] = gelu(
            jnp.dot(tokens[rows, :], carry_weight[...], preferred_element_type=jnp.float32)
        )
        blend[rows, :] = jax.nn.sigmoid(
            jnp.dot(tokens[rows, :], blend_weight[...], preferred_element_type=jnp.float32)
        )
        return carry

    moment_copy = pltpu.make_async_remote_copy(
        src_ref=moments,
        dst_ref=other_moments,
        send_sem=send_moments,
        recv_sem=recv_moments,
        device_id=(me, 1 - core),
        device_id_type=MESH,
    )
    moment_copy.start()
    lax.fori_loop(0, token_tiles, carry_tile, 0)
    small["spatial_gain"].wait()
    small["position_mix"].wait()
    small["position_bias"].wait()
    moment_copy.wait()
    block_head = lax.broadcasted_iota(jnp.int32, (block_length, width), 1) // head_dim
    bias_columns = jnp.concatenate([position_bias[...]] * (8 // heads), axis=0).T
    bias = jnp.zeros((block_length, width), jnp.float32)
    for h in range(heads):
        bias = jnp.where(block_head == h, bias_columns[:, h : h + 1], bias)

    def mix_block(i, carry):
        rows = tile_rows(i, block_length)
        both = (moments[rows, :] + other_moments[rows, :]) * (0.5 / width)
        mean = both[:, :1]
        spread = both[:, 64:65] - mean * mean
        fed = (
            (spatial[rows, :] - mean) * lax.rsqrt(spread + norm_eps) * spatial_gain[...]
        ).astype(jnp.bfloat16)
        every = jnp.dot(position_mix[...], fed, preferred_element_type=jnp.float32)
        found = every[:block_length]
        for h in range(1, heads):
            found = jnp.where(
                block_head == h, every[h * block_length : (h + 1) * block_length], found
            )
        gated[rows, :] = gated[rows, :] * (found + bias)
        return carry

    lax.fori_loop(0, row_count // block_length, mix_block, 0)

    pltpu.make_async_copy(back.at[rest], back.at[rest], recv_part).wait()
    pltpu.make_async_copy(back_logs.at[rest], back_logs.at[rest], recv_log).wait()

    def merge(span):
        owners = [lax.div(ids_smem[k, span], passage_count) for k in range(pick_count)]
        levels = [back_logs[o] for o in owners]
        top = functools.reduce(jnp.maximum, levels)
        scales = [jnp.exp(level - top) for level in levels]
        total = functools.reduce(jnp.add, scales)
        summed = functools.reduce(
            jnp.add, [s * back[o].astype(jnp.float32) for s, o in zip(scales, owners)]
        )
        turned = (summed / total).T
        memory = jnp.concatenate(
            [turned[h * span_length : (h + 1) * span_length] for h in range(heads)], axis=1
        )
        rows = tile_rows(span, span_length)
        return (gated[rows, :] + blend[rows, :] * memory).astype(jnp.bfloat16)

    columns = pl.ds(pl.multiple_of(core * width, width), width)
    half_spans = span_count // 2
    pieces = send_mixed.shape[0]
    per_piece = half_spans // pieces

    def mixed_copy(i):
        rows = tile_rows(i, per_piece * span_length)
        return pltpu.make_async_remote_copy(
            src_ref=mixed.at[rows],
            dst_ref=by_rows.at[rows, columns],
            send_sem=send_mixed.at[i],
            recv_sem=recv_mixed.at[i],
            device_id=(me, 1 - core),
            device_id_type=MESH,
        )

    def merge_theirs(i, carry):
        for k in range(per_piece):
            span = i * per_piece + k
            mixed[tile_rows(span, span_length), :] = merge((1 - core) * half_spans + span)

        @pl.when(i > 0)
        def _():
            mixed_copy(i - 1).start()

        return carry

    lax.fori_loop(0, pieces, merge_theirs, 0)
    mixed_copy(pieces - 1).start()

    piece_rows = per_piece * span_length
    out_columns = 2 * TILE
    small["output_weight"].wait()

    def merge_mine(i, carry):
        for k in range(per_piece):
            span = i * per_piece + k
            by_rows[tile_rows(span, span_length), columns] = merge(core * half_spans + span)
        return carry

    lax.fori_loop(0, pieces, merge_mine, 0)

    def finish(i, carry):
        mixed_copy(i).wait()
        rows = tile_rows(i, piece_rows)
        for n in range(0, out_ref.shape[1], out_columns):
            out_ref[rows, n : n + out_columns] = jnp.dot(
                by_rows[rows, :], output_weight[:, n : n + out_columns], preferred_element_type=jnp.float32
            ).astype(jnp.bfloat16)
        return carry

    lax.fori_loop(0, pieces, finish, 0)
    pltpu.make_async_copy(slots.at[rest], slots.at[rest], send_query).wait()
    pltpu.make_async_copy(table.at[rest], table.at[rest], send_table).wait()
    pltpu.make_async_copy(parts.at[rest], parts.at[rest], send_part).wait()
    pltpu.make_async_copy(logs.at[rest], logs.at[rest], send_log).wait()


def per_device(
    tokens,
    route_ids,
    store,
    token_gain,
    store_gain,
    carry_weight,
    spatial_weight,
    spatial_gain,
    position_mix,
    position_bias,
    query_weight,
    key_weight,
    read_weight,
    blend_weight,
    output_weight,
):
    row_count, features = tokens.shape
    heads, block_length = position_mix.shape[:2]
    width = carry_weight.shape[1]
    span_count = route_ids.shape[0]
    span_length = row_count // span_count
    passage_count, passage_length = store.shape[:2]
    store = store.reshape(passage_count * passage_length, features)
    token_gain = token_gain.reshape(1, features)
    store_gain = store_gain.reshape(1, features)
    spatial_gain = spatial_gain.reshape(1, width)
    position_mix = position_mix.reshape(heads * block_length, block_length)
    bf16, f32 = jnp.bfloat16, jnp.float32
    block = pltpu.VMEM((N_ST, span_length, width), bf16)
    weight = pltpu.VMEM((features, width), bf16)
    by_row = pltpu.VMEM((row_count, width), f32)
    dma = pltpu.SemaphoreType.DMA
    anywhere = pl.BlockSpec(memory_space=pl.ANY)
    return pl.pallas_call(
        layer_kernel,
        out_shape=pltpu.VMEM((row_count // 2, features), bf16),
        in_specs=[
            pl.BlockSpec(memory_space=pltpu.SMEM),
            pl.BlockSpec(memory_space=pltpu.VMEM),
        ]
        + [anywhere] * 14,
        out_specs=pl.BlockSpec(memory_space=pltpu.VMEM),
        scratch_shapes=[
            pltpu.VMEM(tokens.shape, bf16),
            pltpu.VMEM(store.shape, bf16),
            pltpu.VMEM((1, features), f32),
            pltpu.VMEM((1, features), f32),
            weight,
            weight,
            pltpu.VMEM((1, width), f32),
            pltpu.VMEM(position_mix.shape, bf16),
            pltpu.VMEM(position_bias.shape, f32),
            weight,
            weight,
            weight,
            weight,
            pltpu.VMEM(output_weight.shape, bf16),
            pltpu.VMEM((TILE, features), bf16),
            pltpu.VMEM((heads, span_length, width), bf16),
            pltpu.VMEM((span_count, span_length, width), bf16),
            pltpu.VMEM((passage_count, passage_length, width), bf16),
            pltpu.VMEM((passage_count, width, passage_length), bf16),
            block,
            block,
            block,
            block,
            pltpu.VMEM((N_ST, 1, width), f32),
            pltpu.VMEM((N_ST, 1, width), f32),
            pltpu.VMEM((8, 128), f32),
            pltpu.VMEM((1, 128), jnp.int32),
            pltpu.SMEM((1, 128), jnp.int32),
            pltpu.VMEM((1, 128), jnp.int32),
            pltpu.VMEM((N_ST, 1, 128), jnp.int32),
            pltpu.SMEM((N_ST, 1, 128), jnp.int32),
            by_row,
            by_row,
            by_row,
            pltpu.VMEM((row_count, 128), f32),
            pltpu.VMEM((row_count, 128), f32),
            pltpu.VMEM((row_count // 2, width), bf16),
            pltpu.VMEM((row_count // 2, 2 * width), bf16),
            dma((row_count // TILE,)),
            dma((store.shape[0] // TILE,)),
            dma((12,)),
            dma,
            dma((N_ST,)),
        ]
        + [dma] * 8
        + [dma((3,))] * 2
        + [dma] * 2,
        compiler_params=pltpu.CompilerParams(
            collective_id=0, has_side_effects=True, vmem_limit_bytes=60 << 20
        ),
    )(
        route_ids.T,
        route_ids.T,
        tokens,
        store,
        token_gain,
        store_gain,
        carry_weight,
        spatial_weight,
        spatial_gain,
        position_mix,
        position_bias,
        query_weight,
        key_weight,
        read_weight,
        blend_weight,
        output_weight,
    )


def solution(mesh):
    in_specs = (
        P("st", None),
        P("st", None),
        P("st", None, None),
        P(),
        P(),
        P(None, "tp"),
        P(None, "tp"),
        P("tp"),
        P("tp", None, None),
        P("tp", None),
        P(None, "tp"),
        P(None, "tp"),
        P(None, "tp"),
        P(None, "tp"),
        P(),
    )
    out_specs = P(("st", "tp"), None)
    return jax.shard_map(
        per_device, mesh=mesh, in_specs=in_specs, out_specs=out_specs, check_vma=False
    )
```

```python
import functools

import jax
import jax.numpy as jnp
from jax import lax
from jax.experimental import pallas as pl
from jax.experimental.pallas import tpu as pltpu
from jax.sharding import PartitionSpec as P

norm_eps = 1e-06
MESH = pl.DeviceIdType.MESH
SIDE = 4
N_ST = SIDE**3
GROUP = 4
CHUNK = 16
TILE = 256
AHEAD = 8


OFFSETS = [(0, 0, 0)] + [
    ((2 - b + 3 * j) % SIDE, (2 - a + j) % SIDE, j)
    for a in range(SIDE)
    for b in range(SIDE)
    for j in range(SIDE)
    if (a, b, j) != (2, 2, 0)
]


def gelu(x):
    return 0.5 * x * (1.0 + lax.erf(x * 0.5**0.5))


def norm_rows(source, target, gain_ref, count, source_base, target_base, unroll=4):
    features = source.shape[1]
    gain = gain_ref[...]

    def some(i, carry):
        rows = pl.ds(pl.multiple_of(source_base + i * CHUNK, CHUNK), CHUNK)
        values = source[rows, :].astype(jnp.float32)
        mean = jnp.sum(values * values, axis=1, keepdims=True) * (1.0 / features)
        scaled = values * lax.rsqrt(mean + norm_eps) * gain
        rows = pl.ds(pl.multiple_of(target_base + i * CHUNK, CHUNK), CHUNK)
        target[rows, :] = scaled.astype(jnp.bfloat16)
        return carry

    lax.fori_loop(0, count // CHUNK, some, 0, unroll=unroll)


def layer_kernel(
    ids_smem,
    ids_ref,
    tokens_hbm,
    store_hbm,
    token_gain_hbm,
    store_gain_hbm,
    carry_weight_hbm,
    spatial_weight_hbm,
    spatial_gain_hbm,
    position_mix_hbm,
    position_bias_hbm,
    query_weight_hbm,
    key_weight_hbm,
    read_weight_hbm,
    blend_weight_hbm,
    output_weight_hbm,
    out_ref,
    tokens,
    store,
    token_gain,
    store_gain,
    carry_weight,
    spatial_weight,
    spatial_gain,
    position_mix,
    position_bias,
    query_weight,
    key_weight,
    read_weight,
    blend_weight,
    output_weight,
    rows_normed,
    head_mask,
    queries,
    keys,
    values_t,
    slots,
    asked,
    parts,
    back,
    logs,
    back_logs,
    ids_square,
    span_row,
    span_smem,
    local_row,
    table,
    table_smem,
    gated,
    spatial,
    blend,
    moments,
    other_moments,
    mixed,
    own_mixed,
    other_mixed,
    own_product,
    load_tokens,
    load_store,
    load_small,
    send_query,
    recv_query,
    send_table,
    recv_table,
    send_part,
    recv_part,
    send_log,
    recv_log,
    send_moments,
    recv_moments,
    send_mixed,
    recv_mixed,
    span_sem,
    table_sem,
):
    me = lax.axis_index("st")
    core = lax.axis_index("tp")
    pick_count, span_count = ids_ref.shape
    span_length, width = slots.shape[1:]
    passage_count, passage_length = keys.shape[:2]
    heads, block_length = position_bias.shape
    head_dim = width // heads
    row_count = tokens.shape[0]
    my_z, my_y, my_x = lax.div(me, SIDE * SIDE), lax.rem(lax.div(me, SIDE), SIDE), lax.rem(me, SIDE)
    ahead = [
        [lax.rem(digit + d, SIDE) * unit for d in range(SIDE)]
        for digit, unit in ((my_z, SIDE * SIDE), (my_y, SIDE), (my_x, 1))
    ]
    peers = [ahead[0][dz] + ahead[1][dy] + ahead[2][dx] for dz, dy, dx in OFFSETS]

    def sources(group):
        a, b = lax.div(group, SIDE), lax.rem(group, SIDE)
        return [
            lax.rem(my_z + b + j + 2, SIDE) * (SIDE * SIDE)
            + lax.rem(my_y + a + 6 - j, SIDE) * SIDE
            + lax.rem(my_x + SIDE - j, SIDE)
            for j in range(GROUP)
        ]

    def tile_rows(i, size):
        return pl.ds(pl.multiple_of(i * size, size), size)

    def token_load(i):
        rows = tile_rows(i, TILE)
        return pltpu.make_async_copy(tokens_hbm.at[rows], tokens.at[rows], load_tokens.at[i])

    def store_load(i):
        rows = tile_rows(i, TILE)
        return pltpu.make_async_copy(store_hbm.at[rows], store.at[rows], load_store.at[i])

    small = {}
    for n, (name, source, target) in enumerate(
        (
            ("token_gain", token_gain_hbm, token_gain),
            ("query_weight", query_weight_hbm, query_weight),
            ("store_gain", store_gain_hbm, store_gain),
            ("key_weight", key_weight_hbm, key_weight),
            ("read_weight", read_weight_hbm, read_weight),
            ("spatial_weight", spatial_weight_hbm, spatial_weight),
            ("spatial_gain", spatial_gain_hbm, spatial_gain),
            ("carry_weight", carry_weight_hbm, carry_weight),
            ("blend_weight", blend_weight_hbm, blend_weight),
            ("position_mix", position_mix_hbm, position_mix),
            ("position_bias", position_bias_hbm, position_bias),
            ("output_weight", output_weight_hbm, output_weight),
        )
    ):
        small[name] = pltpu.make_async_copy(source, target, load_small.at[n])
    token_tiles = row_count // TILE
    store_tiles = store.shape[0] // TILE
    token_load(0).start()
    small["token_gain"].start()
    small["query_weight"].start()
    for i in range(1, token_tiles):
        token_load(i).start()
    barrier = pltpu.get_barrier_semaphore()
    for peer in peers[1:]:
        pl.semaphore_signal(barrier, inc=1, device_id=(peer, core), device_id_type=MESH)
    pl.semaphore_signal(barrier, inc=1, device_id=(me, 1 - core), device_id_type=MESH)


    def start_later_loads():
        small["store_gain"].start()
        small["key_weight"].start()
        small["read_weight"].start()
        for i in range(store_tiles):
            store_load(i).start()
        for name in (
            "spatial_weight",
            "spatial_gain",
            "carry_weight",
            "blend_weight",
            "position_mix",
            "position_bias",
            "output_weight",
        ):
            small[name].start()

    ids_square[...] = jnp.zeros_like(ids_square)
    ids_square[:pick_count, :span_count] = ids_ref[...].astype(jnp.float32)
    ids = ids_square[...].T[:span_count].astype(jnp.int32)
    lane = lax.broadcasted_iota(jnp.int32, (span_count, 128), 1) * passage_count
    span_index = lax.broadcasted_iota(jnp.int32, (span_count, 128), 0)
    slot_span = jnp.zeros((span_count, 128), jnp.int32)
    slot_local = jnp.zeros((span_count, 128), jnp.int32)
    for k in range(pick_count):
        local = ids[:, k : k + 1] - lane
        hit = (local >= 0) & (local < passage_count)
        slot_span = slot_span + jnp.where(hit, span_index, 0)
        slot_local = slot_local + jnp.where(hit, local, 0)
    slot_span = jnp.sum(slot_span, axis=0, keepdims=True)
    slot_local = jnp.sum(slot_local, axis=0, keepdims=True)
    span_row[...] = jnp.minimum(slot_span, span_count - 1)
    local_row[...] = jnp.minimum(slot_local, passage_count - 1)
    table[me] = local_row[...]
    mask_lane = lax.broadcasted_iota(jnp.int32, (span_length, width), 1) // head_dim
    for h in range(heads):
        head_mask[h] = jnp.where(mask_lane == h, 1.0, 0.0).astype(jnp.bfloat16)
    span_copy = pltpu.make_async_copy(span_row, span_smem, span_sem)
    span_copy.start()

    small["token_gain"].wait()

    def token_query(i):
        found = jnp.dot(
            tokens[i * TILE : (i + 1) * TILE, :], query_weight[...], preferred_element_type=jnp.float32
        ).astype(jnp.bfloat16)
        spans = TILE // span_length
        for s in range(spans):
            queries[i * spans + s] = found[s * span_length : (s + 1) * span_length]

    for i in range(token_tiles):
        token_load(i).wait()
        if i == 1:
            small["query_weight"].wait()
        if i == token_tiles - 1:
            start_later_loads()
        norm_rows(tokens, tokens, token_gain, TILE, i * TILE, i * TILE, TILE // CHUNK if i else 4)
        if i:
            token_query(i - 1)
    token_query(token_tiles - 1)
    span_copy.wait()

    pl.semaphore_wait(barrier, N_ST)

    def table_copy(peer):
        return pltpu.make_async_remote_copy(
            src_ref=local_row,
            dst_ref=table.at[me],
            send_sem=send_table,
            recv_sem=recv_table,
            device_id=(peer, core),
            device_id_type=MESH,
        )

    def query_copy(peer):
        return pltpu.make_async_remote_copy(
            src_ref=slots.at[peer],
            dst_ref=asked.at[me],
            send_sem=send_query,
            recv_sem=recv_query.at[me],
            device_id=(peer, core),
            device_id_type=MESH,
        )

    for peer in peers[1:]:
        table_copy(peer).start()
    for k, peer in enumerate(peers):
        if k > AHEAD:
            query_copy(peers[k - AHEAD]).start()
        slots[peer] = queries[span_smem[0, peer]]
    for peer in peers[N_ST - AHEAD :]:
        query_copy(peer).start()
    asked[me] = slots[me]

    small["store_gain"].wait()
    small["key_weight"].wait()
    small["read_weight"].wait()

    def project(i, carry):
        store_load(i).wait()
        norm_rows(store, rows_normed, store_gain, TILE, i * TILE, 0)
        rows = rows_normed[...]
        key_rows = jnp.dot(rows, key_weight[...], preferred_element_type=jnp.float32)
        value_rows = jnp.dot(rows, read_weight[...], preferred_element_type=jnp.float32)
        several = TILE // passage_length
        for p in range(several):
            part = slice(p * passage_length, (p + 1) * passage_length)
            keys[i * several + p] = key_rows[part].astype(jnp.bfloat16)
            values_t[i * several + p] = value_rows[part].T.astype(jnp.bfloat16)
        return carry

    lax.fori_loop(0, store_tiles, project, 0)

    rest = pl.ds(0, N_ST - 1)
    pltpu.make_async_copy(table.at[rest], table.at[rest], recv_table).wait()
    table_read = pltpu.make_async_copy(table, table_smem, table_sem)
    table_read.start()
    table_read.wait()

    def attend(source):
        index = table_smem[source, 0, me]
        query = asked[source]
        spread = jnp.concatenate([query * head_mask[h] for h in range(heads)], axis=0)
        scores = lax.dot_general(
            keys[index], spread, (((1,), (1,)), ((), ())), preferred_element_type=jnp.float32
        ) * (head_dim**-0.5)
        peak = jnp.max(scores, axis=0, keepdims=True)
        weights = jnp.exp(scores - peak)
        total = jnp.sum(weights, axis=0, keepdims=True)
        summed = jnp.dot(
            values_t[index], weights.astype(jnp.bfloat16), preferred_element_type=jnp.float32
        )
        mine = summed[:head_dim]
        for h in range(1, heads):
            mine = jnp.where(mask_lane == h, summed[h * head_dim : (h + 1) * head_dim], mine)
        return (mine / total).astype(jnp.bfloat16), peak + jnp.log(total)

    def part_copy(source):
        return pltpu.make_async_remote_copy(
            src_ref=parts.at[source],
            dst_ref=back.at[me],
            send_sem=send_part,
            recv_sem=recv_part,
            device_id=(source, core),
            device_id_type=MESH,
        )

    def log_copy(source):
        return pltpu.make_async_remote_copy(
            src_ref=logs.at[source],
            dst_ref=back_logs.at[me],
            send_sem=send_log,
            recv_sem=recv_log,
            device_id=(source, core),
            device_id_type=MESH,
        )

    def send_back(source):
        part_copy(source).start()
        log_copy(source).start()

    def serve(group, carry):
        now = sources(group)
        for source in now:

            @pl.when(source != me)
            def _(source=source):
                pltpu.make_async_copy(asked.at[source], asked.at[source], recv_query.at[source]).wait()

        for source in now:
            part, log_total = attend(source)
            parts[source] = part
            logs[source] = log_total

        @pl.when(group > 0)
        def _():
            send_group(group - 1)

        return carry

    def send_group(group):
        for source in sources(group):

            @pl.when(source != me)
            def _(source=source):
                send_back(source)

    lax.fori_loop(0, N_ST // GROUP, serve, 0)
    send_group(N_ST // GROUP - 1)
    back[me] = parts[me]
    back_logs[me] = logs[me]

    small["spatial_weight"].wait()
    moment_lane = lax.broadcasted_iota(jnp.int32, (TILE, 128), 1)

    def spatial_tile(i, carry):
        rows = tile_rows(i, TILE)
        found = gelu(
            jnp.dot(tokens[rows, :], spatial_weight[...], preferred_element_type=jnp.float32)
        )
        spatial[rows, :] = found
        one = jnp.sum(found, axis=1, keepdims=True)
        two = jnp.sum(found * found, axis=1, keepdims=True)
        moments[rows, :] = jnp.where(moment_lane < 64, one, two)
        return carry

    lax.fori_loop(0, token_tiles, spatial_tile, 0)
    small["carry_weight"].wait()
    small["blend_weight"].wait()

    def carry_tile(i, carry):
        rows = tile_rows(i, TILE)
        gated[rows, :] = gelu(
            jnp.dot(tokens[rows, :], carry_weight[...], preferred_element_type=jnp.float32)
        )
        blend[rows, :] = jax.nn.sigmoid(
            jnp.dot(tokens[rows, :], blend_weight[...], preferred_element_type=jnp.float32)
        )
        return carry

    moment_copy = pltpu.make_async_remote_copy(
        src_ref=moments,
        dst_ref=other_moments,
        send_sem=send_moments,
        recv_sem=recv_moments,
        device_id=(me, 1 - core),
        device_id_type=MESH,
    )
    moment_copy.start()
    lax.fori_loop(0, token_tiles, carry_tile, 0)
    small["spatial_gain"].wait()
    small["position_mix"].wait()
    small["position_bias"].wait()
    moment_copy.wait()
    block_head = lax.broadcasted_iota(jnp.int32, (block_length, width), 1) // head_dim
    bias_columns = jnp.concatenate([position_bias[...]] * (8 // heads), axis=0).T
    bias = jnp.zeros((block_length, width), jnp.float32)
    for h in range(heads):
        bias = jnp.where(block_head == h, bias_columns[:, h : h + 1], bias)

    def mix_block(i, carry):
        rows = tile_rows(i, block_length)
        both = (moments[rows, :] + other_moments[rows, :]) * (0.5 / width)
        mean = both[:, :1]
        spread = both[:, 64:65] - mean * mean
        fed = (
            (spatial[rows, :] - mean) * lax.rsqrt(spread + norm_eps) * spatial_gain[...]
        ).astype(jnp.bfloat16)
        every = jnp.dot(position_mix[...], fed, preferred_element_type=jnp.float32)
        found = every[:block_length]
        for h in range(1, heads):
            found = jnp.where(
                block_head == h, every[h * block_length : (h + 1) * block_length], found
            )
        gated[rows, :] = gated[rows, :] * (found + bias)
        return carry

    lax.fori_loop(0, row_count // block_length, mix_block, 0)

    pltpu.make_async_copy(back.at[rest], back.at[rest], recv_part).wait()
    pltpu.make_async_copy(back_logs.at[rest], back_logs.at[rest], recv_log).wait()

    def merged(span):
        owners = [lax.div(ids_smem[k, span], passage_count) for k in range(pick_count)]
        levels = [back_logs[o] for o in owners]
        top = functools.reduce(jnp.maximum, levels)
        scales = [jnp.exp(level - top) for level in levels]
        total = functools.reduce(jnp.add, scales)
        summed = functools.reduce(
            jnp.add, [s * back[o].astype(jnp.float32) for s, o in zip(scales, owners)]
        )
        return summed / total

    def merge(first):
        turned = jnp.concatenate([merged(first), merged(first + 1)], axis=0).T
        memory = jnp.concatenate(
            [
                jnp.concatenate(
                    [
                        turned[
                            h * span_length : (h + 1) * span_length, s * head_dim : (s + 1) * head_dim
                        ]
                        for h in range(heads)
                    ],
                    axis=1,
                )
                for s in range(2)
            ],
            axis=0,
        )
        rows = pl.ds(pl.multiple_of(first * span_length, 2 * span_length), 2 * span_length)
        return (gated[rows, :] + blend[rows, :] * memory).astype(jnp.bfloat16)

    half_spans = span_count // 2
    pieces = half_spans // 2
    piece_rows = 2 * span_length

    def mixed_copy(i):
        rows = tile_rows(i, piece_rows)
        return pltpu.make_async_remote_copy(
            src_ref=mixed.at[rows],
            dst_ref=other_mixed.at[rows],
            send_sem=send_mixed.at[i],
            recv_sem=recv_mixed.at[i],
            device_id=(me, 1 - core),
            device_id_type=MESH,
        )

    def merge_theirs(i, carry):
        mixed[tile_rows(i, piece_rows), :] = merge((1 - core) * half_spans + 2 * i)

        @pl.when(i > 0)
        def _():
            mixed_copy(i - 1).start()

        return carry

    lax.fori_loop(0, pieces, merge_theirs, 0)
    mixed_copy(pieces - 1).start()

    small["output_weight"].wait()

    def merge_mine(i, carry):
        own_mixed[tile_rows(i, piece_rows), :] = merge(core * half_spans + 2 * i)
        return carry

    lax.fori_loop(0, pieces, merge_mine, 0)

    def product(rows, which, part):
        return jnp.dot(
            rows[...], output_weight[tile_rows(which, width), part], preferred_element_type=jnp.float32
        )

    parts_of_out = [slice(0, out_ref.shape[1])]
    for part in parts_of_out:
        own_product[:, part] = product(own_mixed, core, part)
    for i in range(pieces):
        mixed_copy(i).wait()
    for part in parts_of_out:
        out_ref[:, part] = (own_product[:, part] + product(other_mixed, 1 - core, part)).astype(
            jnp.bfloat16
        )
    pltpu.make_async_copy(slots.at[rest], slots.at[rest], send_query).wait()
    pltpu.make_async_copy(table.at[rest], table.at[rest], send_table).wait()
    pltpu.make_async_copy(parts.at[rest], parts.at[rest], send_part).wait()
    pltpu.make_async_copy(logs.at[rest], logs.at[rest], send_log).wait()


def per_device(
    tokens,
    route_ids,
    store,
    token_gain,
    store_gain,
    carry_weight,
    spatial_weight,
    spatial_gain,
    position_mix,
    position_bias,
    query_weight,
    key_weight,
    read_weight,
    blend_weight,
    output_weight,
):
    row_count, features = tokens.shape
    heads, block_length = position_mix.shape[:2]
    width = carry_weight.shape[1]
    span_count = route_ids.shape[0]
    span_length = row_count // span_count
    passage_count, passage_length = store.shape[:2]
    store = store.reshape(passage_count * passage_length, features)
    token_gain = token_gain.reshape(1, features)
    store_gain = store_gain.reshape(1, features)
    spatial_gain = spatial_gain.reshape(1, width)
    position_mix = position_mix.reshape(heads * block_length, block_length)
    bf16, f32 = jnp.bfloat16, jnp.float32
    block = pltpu.VMEM((N_ST, span_length, width), bf16)
    weight = pltpu.VMEM((features, width), bf16)
    by_row = pltpu.VMEM((row_count, width), f32)
    dma = pltpu.SemaphoreType.DMA
    anywhere = pl.BlockSpec(memory_space=pl.ANY)
    return pl.pallas_call(
        layer_kernel,
        out_shape=pltpu.VMEM((row_count // 2, features), bf16),
        in_specs=[
            pl.BlockSpec(memory_space=pltpu.SMEM),
            pl.BlockSpec(memory_space=pltpu.VMEM),
        ]
        + [anywhere] * 14,
        out_specs=pl.BlockSpec(memory_space=pltpu.VMEM),
        scratch_shapes=[
            pltpu.VMEM(tokens.shape, bf16),
            pltpu.VMEM(store.shape, bf16),
            pltpu.VMEM((1, features), f32),
            pltpu.VMEM((1, features), f32),
            weight,
            weight,
            pltpu.VMEM((1, width), f32),
            pltpu.VMEM(position_mix.shape, bf16),
            pltpu.VMEM(position_bias.shape, f32),
            weight,
            weight,
            weight,
            weight,
            pltpu.VMEM(output_weight.shape, bf16),
            pltpu.VMEM((TILE, features), bf16),
            pltpu.VMEM((heads, span_length, width), bf16),
            pltpu.VMEM((span_count, span_length, width), bf16),
            pltpu.VMEM((passage_count, passage_length, width), bf16),
            pltpu.VMEM((passage_count, width, passage_length), bf16),
            block,
            block,
            block,
            block,
            pltpu.VMEM((N_ST, 1, width), f32),
            pltpu.VMEM((N_ST, 1, width), f32),
            pltpu.VMEM((8, 128), f32),
            pltpu.VMEM((1, 128), jnp.int32),
            pltpu.SMEM((1, 128), jnp.int32),
            pltpu.VMEM((1, 128), jnp.int32),
            pltpu.VMEM((N_ST, 1, 128), jnp.int32),
            pltpu.SMEM((N_ST, 1, 128), jnp.int32),
            by_row,
            by_row,
            by_row,
            pltpu.VMEM((row_count, 128), f32),
            pltpu.VMEM((row_count, 128), f32),
            pltpu.VMEM((row_count // 2, width), bf16),
            pltpu.VMEM((row_count // 2, width), bf16),
            pltpu.VMEM((row_count // 2, width), bf16),
            pltpu.VMEM((row_count // 2, features), f32),
            dma((row_count // TILE,)),
            dma((store.shape[0] // TILE,)),
            dma((12,)),
            dma,
            dma((N_ST,)),
        ]
        + [dma] * 8
        + [dma((3,))] * 2
        + [dma] * 2,
        compiler_params=pltpu.CompilerParams(
            collective_id=0, has_side_effects=True, vmem_limit_bytes=60 << 20
        ),
    )(
        route_ids.T,
        route_ids.T,
        tokens,
        store,
        token_gain,
        store_gain,
        carry_weight,
        spatial_weight,
        spatial_gain,
        position_mix,
        position_bias,
        query_weight,
        key_weight,
        read_weight,
        blend_weight,
        output_weight,
    )


def solution(mesh):
    in_specs = (
        P("st", None),
        P("st", None),
        P("st", None, None),
        P(),
        P(),
        P(None, "tp"),
        P(None, "tp"),
        P("tp"),
        P("tp", None, None),
        P("tp", None),
        P(None, "tp"),
        P(None, "tp"),
        P(None, "tp"),
        P(None, "tp"),
        P(),
    )
    out_specs = P(("st", "tp"), None)
    return jax.shard_map(
        per_device, mesh=mesh, in_specs=in_specs, out_specs=out_specs, check_vma=False
    )
```
